128 devices in a mesh: ep: 32 (over z, y, core), tp: 4 (over x).
Axes of the slice: x: 4, y: 4, z: 4, core: 2. Of those that a mesh axis runs over, the one named last changes fastest.
Arguments:
- tokens: bfloat16 [24576, 2048], P('ep')
- in_gain: float32 [2048], replicated, may hold values from 0.1 to 1.9
- route_ids: int32 [24576, 2], P('ep'), may hold values from 0 to 31, all different within a row; in each aligned block of 768 rows (0 to 767, 768 to 1535, ...) at most 96 rows name the same one
- route_scores: float32 [24576, 2], P('ep'), may hold values from 0.1 to 1
- gate_weight: bfloat16 [32, 2048, 1024], P('ep', None, 'tp'), may hold values from -0.125 to 0.125
- up_weight: bfloat16 [32, 2048, 1024], P('ep', None, 'tp'), may hold values from -0.125 to 0.125
- down_weight: bfloat16 [32, 1024, 2048], P('ep', 'tp')
- out_gain: float32 [2048], P('tp'), may hold values from 0.1 to 1.9
Outputs:
- mixed: bfloat16 [24576, 2048], P('ep', 'tp')
The draws below stay inside these ranges and needn't reach their ends.
Inputs may be any that keep to these rules, and one draw needn't show every extreme that they name: `route_ids`: each row names 2 different experts. Among the rows of one index of ep (aligned blocks of 768 rows) no expert is named more than 96 times, a bound that some block reaches.
All inputs are finite; a program needn't handle non-finite values.
Results may differ from the reference program's by a relative error of at most 0.012.
Values may be sent and summed in bfloat16 or wider, within the bound.
No kernel may reach another device: no remote copies, remote signals or barrier semaphores. Data moves between devices by JAX's collectives and lax.ppermute only.
A program may use at most 128 MiB of HBM per device.

```python
import math
import jax
import jax.numpy as jnp
import numpy as np
from jax import lax

D = 2048
FF = 1024
TOP_K = 2
TOK_DEV = 768
EXPERTS = 32
TOKENS = 24576
CAP = 96
FF_PART = 256
N_EP = 32
N_TP = 4


def draw_tokens(key, part):
    keys = jax.random.split(jax.random.fold_in(key, 3), 3)
    row_scale = 10.0 ** jax.random.uniform(keys[1], (TOKENS, 1), jnp.float32)
    column_scale = 10.0 ** (0.5 * jax.random.uniform(keys[2], (1, D), jnp.float32))
    values = jax.random.normal(keys[0], (TOKENS, D), jnp.float32) * row_scale * column_scale
    return values.astype(jnp.bfloat16)


def draw_down_weight(key, part):
    keys = jax.random.split(jax.random.fold_in(key, 11), 2)
    position = jnp.arange(D, dtype=jnp.float32) / D
    base = jax.random.normal(keys[0], (EXPERTS, FF, D), jnp.float32)
    scale = 10.0 ** (0.5 * position + 0.5 * jax.random.uniform(keys[1], (D,), jnp.float32))
    return (base * FF ** (-0.5) * scale[None, None, :]).astype(jnp.bfloat16)


def steps_of(stream_key, dims, pieces, smallest, top_value):
    loudness = 1.0
    for dim, parts in pieces:
        draws = jax.random.uniform(jax.random.fold_in(jax.random.fold_in(stream_key, 6), dim), (parts,), jnp.float32, smallest / len(pieces), top_value / len(pieces))
        loudness = loudness * jnp.repeat(jnp.exp(draws), dims[dim] // parts).reshape((-1,) + (1,) * (len(dims) - 1 - dim))
    return loudness


def routed_block(own_key, own, number, rows, count, top, reach, lean):
    sequence = jax.random.permutation(own_key, count)
    crowded, usual = shares(count, rows * top, reach, lean, True), shares(count, rows * top, reach, lean, False)
    places = jnp.arange(count)

    def named(tallies, rotation):
        used = int((tallies > 0).sum())
        fixed = max(1, used // 4)
        moved = fixed + (places - fixed + rotation * (used - fixed)) % max(1, count - fixed)
        return jnp.zeros((count,), jnp.int32).at[sequence[jnp.where(places < fixed, places, moved)]].set(jnp.asarray(tallies, jnp.int32))

    tallies = jnp.where(number % 4 == 0, named(crowded, number // 4), named(usual, number - number // 4 - 1))
    mixed = jax.random.permutation(jax.random.fold_in(own, 3), count)
    giver, sink = mixed[0:count // 2 * 2:2], mixed[1:count // 2 * 2:2]
    margin = jnp.minimum(tallies[giver] - 1, reach - tallies[sink]) // 2
    margin = jnp.where((giver == sequence[0]) | (sink == sequence[0]) | (tallies[sink] == 0), 0, jnp.maximum(margin, 0))
    moved = jax.random.randint(jax.random.fold_in(own, 4), (count // 2,), 0, 1 << 20) % (margin + 1)
    tallies = tallies.at[giver].add(-moved).at[sink].add(moved)
    labels = jnp.searchsorted(jnp.cumsum(tallies), jnp.arange(rows * top), side="right").astype(jnp.int32)
    listing = labels.reshape(top, rows).T
    listing = listing[jax.random.permutation(jax.random.fold_in(own, 1), rows)]
    rotation = jax.random.randint(jax.random.fold_in(own, 2), (rows, 1), 0, top)
    return jnp.take_along_axis(listing, (jnp.arange(top)[None, :] + rotation) % top, axis=1)


def shares(count, total, most, slope, full):
    weights = [(1 << 20) // math.isqrt(standing ** slope) + 1 for standing in range(1, count + 1)]
    largest = most if full else min(most, max(-(-total // count), total * weights[0] // sum(weights)))
    least = 1 if total - largest >= count - 1 else 0
    counts, spare = [largest] + [least] * (count - 1), total - largest - least * (count - 1)
    while spare > 0:
        candidates = [i for i in range(1, count) if counts[i] < largest] or [i for i in range(1, count) if counts[i] < most]
        pool, left = sum([weights[i] for i in candidates]), spare
        for i in candidates:
            addition = min(most - counts[i], max(1, left * weights[i] // pool), spare)
            counts[i] = counts[i] + addition
            spare = spare - addition
    return np.array(counts)


def noise(stream_key, shape, scale, most, cuts=(), kind=jnp.bfloat16):
    values = scale * jax.random.normal(stream_key, shape, jnp.float32)
    if cuts:
        values = values * steps_of(stream_key, shape, cuts, -0.22, 0.18)
    return jnp.clip(values, -most, most).astype(kind)


def setup_inputs(seed: int = 0) -> dict:
    key_of = jax.random.split(jax.random.key(seed), 9)
    tokens = draw_tokens(jax.random.fold_in(key_of[8], 71), 0)
    in_gain = jnp.clip(1.0 + 0.18 * jax.random.normal(key_of[1], (D,), jnp.float32), 0.1, 1.9)
    route_ids_keys = jax.random.split(jax.random.fold_in(key_of[2], 1), TOKENS // TOK_DEV)
    route_ids_turns = jax.random.permutation(jax.random.fold_in(key_of[2], 3), TOKENS // TOK_DEV)
    route_ids = jax.vmap(lambda own, number: routed_block(jax.random.fold_in(key_of[2], 2), own, number, TOK_DEV, EXPERTS, TOP_K, CAP, 2))(route_ids_keys, route_ids_turns).reshape((TOKENS, TOP_K))
    route_scores = jnp.clip(jnp.exp(math.log(1.0) - 2.3025851 * jax.random.uniform(key_of[3], (TOKENS, TOP_K), jnp.float32) ** steps_of(key_of[3], (TOKENS, TOP_K), ((0, 32),), -0.2, 0.2)), 0.1, 1.0)
    gate_weight = noise(key_of[4], (EXPERTS, D, FF), D ** -0.5, 0.125, ((0, 32), (2, 4)))
    up_weight = noise(key_of[5], (EXPERTS, D, FF), D ** -0.5, 0.125, ((0, 32), (2, 4)))
    down_weight = draw_down_weight(jax.random.fold_in(key_of[8], 71), 0)
    out_gain = jnp.clip(1.0 + 0.18 * jax.random.normal(key_of[7], (D,), jnp.float32), 0.1, 1.9)
    return dict(tokens=tokens, in_gain=in_gain, route_ids=route_ids, route_scores=route_scores, gate_weight=gate_weight, up_weight=up_weight, down_weight=down_weight, out_gain=out_gain)


epsilon = 1e-06

def reference(tokens, in_gain, route_ids, route_scores, gate_weight, up_weight, down_weight, out_gain):
    as_float = tokens.astype(jnp.float32)
    normed = (as_float * lax.rsqrt(lax.optimization_barrier(jnp.mean(as_float * as_float, axis=1, keepdims=True)) + epsilon) * in_gain).astype(jnp.bfloat16)
    flat_ids = route_ids.reshape(N_EP, TOK_DEV * TOP_K)
    one_hot = (flat_ids[:, :, None] == jnp.arange(EXPERTS, dtype=jnp.int32)[None, None, :]).astype(jnp.int32)
    slot_index = lax.optimization_barrier(jnp.sum((jnp.cumsum(one_hot, axis=1) - 1) * one_hot, axis=2)).astype(jnp.int32)
    block_index = jnp.broadcast_to(jnp.arange(N_EP, dtype=jnp.int32)[:, None], flat_ids.shape)
    row_index = (block_index * TOK_DEV + jnp.arange(TOK_DEV * TOP_K, dtype=jnp.int32)[None, :] // TOP_K).astype(jnp.int32)
    buffer = jnp.zeros((EXPERTS, N_EP, CAP, D), jnp.bfloat16)
    buffer = buffer.at[flat_ids, block_index, slot_index].set(normed[row_index])

    def expert_run(inputs):
        rows_in, gate_w, up_w, down_w = inputs
        gate_acts = jnp.dot(rows_in, gate_w, preferred_element_type=jnp.float32)
        up_acts = jnp.dot(rows_in, up_w, preferred_element_type=jnp.float32)
        hidden = (jax.nn.silu(gate_acts) * up_acts).astype(jnp.bfloat16)
        hidden_blocks = hidden.reshape(-1, N_TP, FF_PART).astype(jnp.float32)
        down_blocks = down_w.reshape(N_TP, FF_PART, D).astype(jnp.float32)
        partial_value = jnp.einsum('rpf,pfd->prd', hidden_blocks, down_blocks)
        rounded = lax.optimization_barrier(partial_value.astype(jnp.bfloat16))
        return lax.optimization_barrier(jnp.sum(rounded.astype(jnp.float32), axis=0)).astype(jnp.bfloat16)
    outputs = lax.map(expert_run, (buffer.reshape(EXPERTS, N_EP * CAP, D), gate_weight, up_weight, down_weight))
    outputs = outputs.reshape(EXPERTS, N_EP, CAP, D)
    picked = outputs[flat_ids, block_index, slot_index].astype(jnp.float32).reshape(TOKENS, TOP_K, D)
    mix_weight = route_scores / lax.optimization_barrier(jnp.sum(route_scores, axis=1, keepdims=True))
    combined = lax.optimization_barrier(jnp.sum(mix_weight[:, :, None] * picked, axis=1))
    mixed = combined * lax.rsqrt(lax.optimization_barrier(jnp.mean(combined * combined, axis=1, keepdims=True)) + epsilon) * out_gain
    return mixed.astype(jnp.bfloat16)
```

```python
import functools

import jax
import jax.numpy as jnp
from jax import lax
from jax.experimental import pallas as pl
from jax.experimental.pallas import tpu as pltpu
from jax.sharding import PartitionSpec as P

epsilon = 1e-06
AXES = ("ep", "tp")
VMEM_BYTES = 58 * 1024 * 1024


def place_of(ids, slot):
    ep = (ids // 2) * 2 + slot % 2
    tp = (ids % 2) * 2 + (slot % 4) // 2
    return ep, tp, slot // 4


def permutes(count_ep, count_tp):
    def dev(ep, x):
        return ep * count_tp + x

    first, second, swap = [], [], []
    for ep in range(count_ep):
        core = ep % 2
        for x in range(count_tp):
            own = x // 2 == core
            swap.append((dev(ep, x), dev(ep ^ 1, x)))
            if own:
                first.append((dev(ep, x), dev(ep, x ^ 1)))
                second.append((dev(ep, x), dev(ep, x)))
            else:
                first.append((dev(ep, x), dev(ep ^ 1, count_tp - 1 - x)))
                second.append((dev(ep, x), dev(ep, x ^ 1)))
    return first, second, swap


def dispatch_kernel(where_ref, ids_ref, gain_ref, tokens_ref, out_ref, raw, normed, pick, sems, *, rows, chunks):
    step = pl.program_id(0)
    count, width = raw.shape
    part = count // chunks

    @pl.when(step == 0)
    def _():
        for i in range(chunks):
            pltpu.make_async_copy(
                tokens_ref.at[pl.ds(i * part, part)], raw.at[pl.ds(i * part, part)], sems.at[i]
            ).start()
        experts = 32
        first = ids_ref[0:1, :]
        second = ids_ref[1:2, :]
        number = lax.broadcasted_iota(jnp.int32, (experts, count), 0)
        named_first = number == first
        named_second = number == second
        named = jnp.where(named_first | named_second, 1.0, 0.0).astype(jnp.bfloat16)
        before = lax.broadcasted_iota(jnp.int32, (count, count), 0) < lax.broadcasted_iota(
            jnp.int32, (count, count), 1
        )
        ranks = jnp.dot(
            named, jnp.where(before, 1.0, 0.0).astype(jnp.bfloat16), preferred_element_type=jnp.float32
        )
        slot_first = jnp.sum(jnp.where(named_first, ranks, 0.0), axis=0, keepdims=True).astype(jnp.int32)
        slot_second = jnp.sum(jnp.where(named_second, ranks, 0.0), axis=0, keepdims=True).astype(jnp.int32)
        mine = where_ref[0]

        def row_of(ids, slot):
            ep, tp, row = place_of(ids, slot)
            return jnp.where(tp == mine, ep * rows + row, -1)

        row_first = row_of(first, slot_first)
        row_second = row_of(second, slot_second)
        index = lax.broadcasted_iota(jnp.int32, (count, count), 0)
        pick[...] = jnp.where((index == row_first) | (index == row_second), 1.0, 0.0).astype(jnp.bfloat16)
        gain = gain_ref[...]
        for i in range(chunks):
            pltpu.make_async_copy(
                tokens_ref.at[pl.ds(i * part, part)], raw.at[pl.ds(i * part, part)], sems.at[i]
            ).wait()
            value = raw[pl.ds(i * part, part), :].astype(jnp.float32)
            mean = jnp.mean(value * value, axis=1, keepdims=True)
            normed[pl.ds(i * part, part), :] = (value * lax.rsqrt(mean + epsilon) * gain).astype(jnp.bfloat16)

    block = out_ref.shape[0]
    out_ref[...] = jnp.dot(
        pick[pl.ds(step * block, block), :], normed[...], preferred_element_type=jnp.float32
    ).astype(jnp.bfloat16)


def dispatch_buffer(place, ids_rows, gain, tokens, rows):
    count, width = tokens.shape
    steps, chunks = 4, 4
    return pl.pallas_call(
        functools.partial(dispatch_kernel, rows=rows, chunks=chunks),
        grid_spec=pltpu.PrefetchScalarGridSpec(
            num_scalar_prefetch=1,
            grid=(steps,),
            in_specs=[
                pl.BlockSpec((2, count), lambda i, p: (0, 0)),
                pl.BlockSpec((1, width), lambda i, p: (0, 0)),
                pl.BlockSpec(memory_space=pl.ANY),
            ],
            out_specs=pl.BlockSpec((count // steps, width), lambda i, p: (i, 0)),
            scratch_shapes=[
                pltpu.VMEM((count, width), jnp.bfloat16),
                pltpu.VMEM((count, width), jnp.bfloat16),
                pltpu.VMEM((count, count), jnp.bfloat16),
                pltpu.SemaphoreType.DMA((chunks,)),
            ],
        ),
        out_shape=jax.ShapeDtypeStruct((count, width), jnp.bfloat16),
        compiler_params=pltpu.CompilerParams(
            dimension_semantics=("arbitrary",), vmem_limit_bytes=VMEM_BYTES
        ),
        name="dispatch_buffer",
    )(place, ids_rows, gain, tokens)


def hidden_of(rows, gate, up):
    gate_acts = jnp.dot(rows, gate, preferred_element_type=jnp.float32)
    up_acts = jnp.dot(rows, up, preferred_element_type=jnp.float32)
    return (gate_acts / (1.0 + jnp.exp(-gate_acts)) * up_acts).astype(jnp.bfloat16)


def early_kernel(place_ref, rows_ref, ga, gb, g1, g2, ua, ub, u1, u2, out_ref, rows, gate, up, sems):
    flag = place_ref[1]

    def copies(a, b, dst, sem):
        @pl.when(flag == 1)
        def _():
            pltpu.make_async_copy(a, dst, sem).start()

        @pl.when(flag != 1)
        def _():
            pltpu.make_async_copy(b, dst, sem).start()

    copies(ga, gb, gate.at[0], sems.at[0])
    copies(ua, ub, up.at[0], sems.at[1])
    load = pltpu.make_async_copy(rows_ref, rows, sems.at[6])
    load.start()
    for i, (g, u) in enumerate(((g1, u1), (g2, u2))):
        pltpu.make_async_copy(g, gate.at[i + 1], sems.at[2 * i + 2]).start()
        pltpu.make_async_copy(u, up.at[i + 1], sems.at[2 * i + 3]).start()
    load.wait()
    part = gate.shape[2]
    for i in range(3):
        pltpu.make_async_copy(g1, gate.at[i], sems.at[2 * i]).wait()
        pltpu.make_async_copy(u1, up.at[i], sems.at[2 * i + 1]).wait()
        out_ref[:, i * part : (i + 1) * part] = hidden_of(rows[...], gate[i], up[i])


def early_hidden(place, rows, gates, ups):
    count, width = rows.shape
    part = gates[0].shape[1]
    any_spec = pl.BlockSpec(memory_space=pl.ANY)
    return pl.pallas_call(
        early_kernel,
        in_specs=[pl.BlockSpec(memory_space=pltpu.SMEM)] + [any_spec] * 9,
        out_specs=pl.BlockSpec((count, 3 * part), lambda: (0, 0)),
        scratch_shapes=[
            pltpu.VMEM((count, width), jnp.bfloat16),
            pltpu.VMEM((3, width, part), jnp.bfloat16),
            pltpu.VMEM((3, width, part), jnp.bfloat16),
            pltpu.SemaphoreType.DMA((7,)),
        ],
        out_shape=jax.ShapeDtypeStruct((count, 3 * part), jnp.bfloat16),
        compiler_params=pltpu.CompilerParams(vmem_limit_bytes=VMEM_BYTES),
        name="early_hidden",
    )(place, rows, *gates, *ups)


def late_kernel(
    place_ref, rows_ref, early_ref, ga, gb, ua, ub, d0a, d0b, d1, d2, d3a, d3b, out_ref, rows, gate, up, down, hidden, sems, *, slots
):
    flag = place_ref[1]

    def copies(a, b, dst, sem):
        @pl.when(flag == 1)
        def _():
            pltpu.make_async_copy(a, dst, sem).start()

        @pl.when(flag != 1)
        def _():
            pltpu.make_async_copy(b, dst, sem).start()

    load = pltpu.make_async_copy(rows_ref, rows, sems.at[0])
    load.start()
    copies(ga, gb, gate, sems.at[1])
    copies(ua, ub, up, sems.at[2])
    part = gate.shape[1]
    copies(d0a, d0b, down.at[pl.ds(0, part)], sems.at[3])
    pltpu.make_async_copy(d1, down.at[pl.ds(part, part)], sems.at[4]).start()
    pltpu.make_async_copy(d2, down.at[pl.ds(2 * part, part)], sems.at[5]).start()
    copies(d3a, d3b, down.at[pl.ds(3 * part, part)], sems.at[6])
    pre = pltpu.make_async_copy(early_ref, hidden.at[:, pl.ds(0, 3 * part)], sems.at[7])
    pre.start()
    load.wait()
    pltpu.make_async_copy(ga, gate, sems.at[1]).wait()
    pltpu.make_async_copy(ua, up, sems.at[2]).wait()
    hidden[:, 3 * part : 4 * part] = hidden_of(rows[...], gate[...], up[...])
    for i in range(4):
        pltpu.make_async_copy(d1, down.at[pl.ds(i * part, part)], sems.at[3 + i]).wait()
    pre.wait()
    senders, pieces, _, piece = out_ref.shape
    for f in range(pieces):
        value = jnp.dot(
            hidden[...], down[:, f * piece : (f + 1) * piece], preferred_element_type=jnp.float32
        )
        out_ref[:, f] = value.reshape(senders, slots, piece).astype(jnp.bfloat16)


def late_outputs(place, rows, early, gates, ups, downs, senders, pieces):
    count, width = rows.shape
    part = gates[0].shape[1]
    slots = count // senders
    any_spec = pl.BlockSpec(memory_space=pl.ANY)
    shape = (senders, pieces, slots, width // pieces)
    return pl.pallas_call(
        functools.partial(late_kernel, slots=slots),
        in_specs=[pl.BlockSpec(memory_space=pltpu.SMEM)] + [any_spec] * 12,
        out_specs=pl.BlockSpec(shape, lambda: (0, 0, 0, 0)),
        scratch_shapes=[
            pltpu.VMEM((count, width), jnp.bfloat16),
            pltpu.VMEM((width, part), jnp.bfloat16),
            pltpu.VMEM((width, part), jnp.bfloat16),
            pltpu.VMEM((4 * part, width), jnp.bfloat16),
            pltpu.VMEM((count, 4 * part), jnp.bfloat16),
            pltpu.SemaphoreType.DMA((8,)),
        ],
        out_shape=jax.ShapeDtypeStruct(shape, jnp.bfloat16),
        compiler_params=pltpu.CompilerParams(vmem_limit_bytes=VMEM_BYTES),
        name="late_outputs",
    )(place, rows, early, *gates, *ups, *downs)


def columns_kernel(ids_ref, out_ref, *, rows, count_tp):
    count = ids_ref.shape[0]
    experts = 32
    first = ids_ref[:, 0:1]
    second = ids_ref[:, 1:2]
    number = lax.broadcasted_iota(jnp.int32, (count, experts), 1)
    named_first = number == first
    named_second = number == second
    named = jnp.where(named_first | named_second, 1.0, 0.0).astype(jnp.bfloat16)
    before = lax.broadcasted_iota(jnp.int32, (count, count), 1) < lax.broadcasted_iota(
        jnp.int32, (count, count), 0
    )
    ranks = jnp.dot(
        jnp.where(before, 1.0, 0.0).astype(jnp.bfloat16), named, preferred_element_type=jnp.float32
    )

    def row_of(ids, chosen):
        slot = jnp.sum(jnp.where(chosen, ranks, 0.0), axis=1, keepdims=True).astype(jnp.int32)
        ep, tp, row = place_of(ids, slot)
        return (ep * count_tp + tp) * rows + row

    out_ref[:, 0:1] = row_of(first, named_first)
    out_ref[:, 1:2] = row_of(second, named_second)


def combine_kernel(index_ref, scores_ref, returned_ref, out_ref):
    total = returned_ref.shape[0]
    count = index_ref.shape[0]
    index = lax.broadcasted_iota(jnp.int32, (count, total), 1)
    returned = returned_ref[...]

    def picked(choice):
        hot = jnp.where(index == index_ref[:, choice : choice + 1], 1.0, 0.0).astype(jnp.bfloat16)
        return jnp.dot(hot, returned, preferred_element_type=jnp.float32)

    scores = scores_ref[...]
    mix = scores / jnp.sum(scores, axis=1, keepdims=True)
    out_ref[...] = mix[:, 0:1] * picked(0) + mix[:, 1:2] * picked(1)


def combine(index, scores, returned):
    count = index.shape[0]
    total, piece = returned.shape
    steps = 4
    return pl.pallas_call(
        combine_kernel,
        grid=(steps,),
        in_specs=[
            pl.BlockSpec((count // steps, 2), lambda i: (i, 0)),
            pl.BlockSpec((count // steps, 2), lambda i: (i, 0)),
            pl.BlockSpec((total, piece), lambda i: (0, 0)),
        ],
        out_specs=pl.BlockSpec((count // steps, piece), lambda i: (i, 0)),
        out_shape=jax.ShapeDtypeStruct((count, piece), jnp.float32),
        compiler_params=pltpu.CompilerParams(
            dimension_semantics=("arbitrary",), vmem_limit_bytes=VMEM_BYTES
        ),
        name="combine",
    )(index, scores, returned)


def per_device(
    tokens, in_gain, route_ids, route_scores, gate_weight, up_weight, down_weight, out_gain
):
    count_ep = lax.axis_size("ep")
    count_tp = lax.axis_size("tp")
    tok_count, full_width = tokens.shape
    part_width = full_width // count_tp
    capacity = 2 * tok_count * route_ids.shape[1] // count_ep
    rows = capacity // count_tp
    x = lax.axis_index("tp")
    core = lax.axis_index("ep") % 2
    place = jnp.stack([x, (x // 2 == core).astype(jnp.int32)]).astype(jnp.int32)

    first, second, swap = permutes(count_ep, count_tp)

    def spread(weight):
        moved = lax.ppermute(weight, AXES, first)
        other_own = lax.ppermute(weight, AXES, swap)
        other_moved = lax.ppermute(moved, AXES, swap)
        last = lax.ppermute(moved, AXES, second)
        other_last = lax.ppermute(last, AXES, swap)
        return (weight, other_own), moved, other_moved, (other_last, last)

    gate = spread(gate_weight[0])
    up = spread(up_weight[0])
    down = spread(down_weight[0])

    buffer = dispatch_buffer(place, route_ids.T, in_gain[None, :], tokens, rows)
    received = lax.all_to_all(
        buffer.reshape(count_ep, rows, full_width), "ep", split_axis=0, concat_axis=0, tiled=True
    ).reshape(count_ep * rows, full_width)
    early = early_hidden(
        place, received, (*gate[0], gate[1], gate[2]), (*up[0], up[1], up[2])
    )
    outputs = late_outputs(
        place, received, early, gate[3], up[3], (*down[0], down[1], down[2], *down[3]), count_ep, count_tp
    )
    returned = lax.all_to_all(
        outputs.reshape(count_ep * count_tp, rows, part_width), AXES, split_axis=0, concat_axis=0, tiled=True
    ).reshape(count_ep * count_tp * rows, part_width)
    index = pl.pallas_call(
        functools.partial(columns_kernel, rows=rows, count_tp=count_tp),
        out_shape=jax.ShapeDtypeStruct((tok_count, 2), jnp.int32),
        name="columns",
    )(route_ids)
    combined = combine(index, route_scores, returned)
    squares = jnp.sum(combined * combined, axis=1)
    total = squares
    for shift in range(1, count_tp):
        total = total + lax.ppermute(
            squares, "tp", [(i, (i + shift) % count_tp) for i in range(count_tp)]
        )
    scaled = combined * lax.rsqrt(total[:, None] / full_width + epsilon) * out_gain
    return scaled.astype(jnp.bfloat16)


def solution(mesh):
    in_specs = (
        P("ep", None),
        P(),
        P("ep", None),
        P("ep", None),
        P("ep", None, "tp"),
        P("ep", None, "tp"),
        P("ep", "tp", None),
        P("tp"),
    )
    out_specs = P("ep", "tp")
    return jax.shard_map(
        per_device, mesh=mesh, in_specs=in_specs, out_specs=out_specs, check_vma=False
    )
```

```python
import functools

import jax
import jax.numpy as jnp
from jax import lax
from jax.experimental import pallas as pl
from jax.experimental.pallas import tpu as pltpu
from jax.sharding import PartitionSpec as P


epsilon = 1e-06
AXES = ("ep", "tp")
MIB = 1024 * 1024


def place_of(ids, slot):
    ep = (ids // 2) * 2 + slot % 2
    tp = (ids % 2) * 2 + (slot % 4) // 2
    return ep, tp, slot // 4


def permutes(count_ep, count_tp):
    def dev(ep, x):
        return ep * count_tp + x

    first, second, swap = [], [], []
    for ep in range(count_ep):
        core = ep % 2
        for x in range(count_tp):
            own = x // 2 == core
            swap.append((dev(ep, x), dev(ep ^ 1, x)))
            if own:
                first.append((dev(ep, x), dev(ep, x ^ 1)))
            else:
                first.append((dev(ep, x), dev(ep ^ 1, count_tp - 1 - x)))
                second.append((dev(ep, x), dev(ep, x ^ 1)))
    return first, second, swap


def dispatch_kernel(where_ref, ids_ref, gain_ref, tokens_ref, out_ref, raw, normed, pick, sems, *, rows, chunks):
    step = pl.program_id(0)
    count, _ = raw.shape
    part = count // chunks

    @pl.when(step == 0)
    def _():
        for i in range(chunks):
            pltpu.make_async_copy(
                tokens_ref.at[pl.ds(i * part, part)], raw.at[pl.ds(i * part, part)], sems.at[i]
            ).start()
        experts = 32
        first = ids_ref[0:1, :]
        second = ids_ref[1:2, :]
        number = lax.broadcasted_iota(jnp.int32, (experts, count), 0)
        named_first = number == first
        named_second = number == second
        named = jnp.where(named_first | named_second, 1.0, 0.0).astype(jnp.bfloat16)
        before = lax.broadcasted_iota(jnp.int32, (count, count), 0) < lax.broadcasted_iota(
            jnp.int32, (count, count), 1
        )
        ranks = jnp.dot(
            named, jnp.where(before, 1.0, 0.0).astype(jnp.bfloat16), preferred_element_type=jnp.float32
        )
        slot_first = jnp.sum(jnp.where(named_first, ranks, 0.0), axis=0, keepdims=True).astype(jnp.int32)
        slot_second = jnp.sum(jnp.where(named_second, ranks, 0.0), axis=0, keepdims=True).astype(jnp.int32)
        mine = where_ref[0]

        def row_of(ids, slot):
            ep, tp, row = place_of(ids, slot)
            return jnp.where(tp == mine, ep * rows + row, -1)

        row_first = row_of(first, slot_first)
        row_second = row_of(second, slot_second)
        index = lax.broadcasted_iota(jnp.int32, (count, count), 0)
        pick[...] = jnp.where((index == row_first) | (index == row_second), 1.0, 0.0).astype(jnp.bfloat16)
        gain = gain_ref[...]
        for i in range(chunks):
            pltpu.make_async_copy(
                tokens_ref.at[pl.ds(i * part, part)], raw.at[pl.ds(i * part, part)], sems.at[i]
            ).wait()
            value = raw[pl.ds(i * part, part), :].astype(jnp.float32)
            mean = jnp.mean(value * value, axis=1, keepdims=True)
            normed[pl.ds(i * part, part), :] = (value * lax.rsqrt(mean + epsilon) * gain).astype(jnp.bfloat16)

    block = out_ref.shape[0]
    out_ref[...] = jnp.dot(
        pick[pl.ds(step * block, block), :], normed[...], preferred_element_type=jnp.float32
    ).astype(jnp.bfloat16)


def dispatch_buffer(place, ids_rows, gain, tokens, rows):
    count, width = tokens.shape
    steps, chunks = 4, 4
    return pl.pallas_call(
        functools.partial(dispatch_kernel, rows=rows, chunks=chunks),
        grid_spec=pltpu.PrefetchScalarGridSpec(
            num_scalar_prefetch=1,
            grid=(steps,),
            in_specs=[
                pl.BlockSpec((2, count), lambda i, p: (0, 0)),
                pl.BlockSpec((1, width), lambda i, p: (0, 0)),
                pl.BlockSpec(memory_space=pltpu.HBM),
            ],
            out_specs=pl.BlockSpec((count // steps, width), lambda i, p: (i, 0)),
            scratch_shapes=[
                pltpu.VMEM((count, width), jnp.bfloat16),
                pltpu.VMEM((count, width), jnp.bfloat16),
                pltpu.VMEM((count, count), jnp.bfloat16),
                pltpu.SemaphoreType.DMA((chunks,)),
            ],
        ),
        out_shape=pltpu.HBM((count, width), jnp.bfloat16),
        compiler_params=pltpu.CompilerParams(
            dimension_semantics=("arbitrary",), vmem_limit_bytes=58 * MIB
        ),
        name="dispatch_buffer",
    )(place, ids_rows, gain, tokens)


def hidden_of(rows, gate, up):
    gate_acts = jnp.dot(rows, gate, preferred_element_type=jnp.float32)
    up_acts = jnp.dot(rows, up, preferred_element_type=jnp.float32)
    return gate_acts / (1.0 + jnp.exp(-gate_acts)) * up_acts


def start_one(flag, a, b, dst, sem):
    @pl.when(flag == 1)
    def _():
        pltpu.make_async_copy(a, dst, sem).start()

    @pl.when(flag != 1)
    def _():
        pltpu.make_async_copy(b, dst, sem).start()


def early_kernel(place_ref, rows_ref, ga, gb, g1, g2, ua, ub, u1, u2, out_ref, rows, gate, up, sems):
    flag = place_ref[1]
    start_one(flag, ga, gb, gate.at[0], sems.at[0])
    start_one(flag, ua, ub, up.at[0], sems.at[1])
    load = pltpu.make_async_copy(rows_ref, rows, sems.at[6])
    load.start()
    for i, (g, u) in enumerate(((g1, u1), (g2, u2))):
        pltpu.make_async_copy(g, gate.at[i + 1], sems.at[2 * i + 2]).start()
        pltpu.make_async_copy(u, up.at[i + 1], sems.at[2 * i + 3]).start()
    load.wait()
    part = gate.shape[2]
    for i in range(3):
        pltpu.make_async_copy(g1, gate.at[i], sems.at[2 * i]).wait()
        pltpu.make_async_copy(u1, up.at[i], sems.at[2 * i + 1]).wait()
        value = hidden_of(rows[...], gate[i], up[i])
        out_ref[:, i * part : (i + 1) * part] = value.astype(jnp.bfloat16)


def middle_kernel(place_ref, rows_ref, ga, gb, ua, ub, out_ref, rows, gate, up, sems):
    flag = place_ref[1]
    load = pltpu.make_async_copy(rows_ref, rows, sems.at[0])
    load.start()
    start_one(flag, ga, gb, gate, sems.at[1])
    start_one(flag, ua, ub, up, sems.at[2])
    load.wait()
    pltpu.make_async_copy(ga, gate, sems.at[1]).wait()
    pltpu.make_async_copy(ua, up, sems.at[2]).wait()
    out_ref[...] = hidden_of(rows[...], gate[...], up[...]).astype(jnp.bfloat16)


HBM = pl.BlockSpec(memory_space=pltpu.HBM)
ANY = pl.BlockSpec(memory_space=pl.ANY)
SMEM = pl.BlockSpec(memory_space=pltpu.SMEM)


def early_hidden(place, rows, gates, ups):
    count, width = rows.shape
    part = gates[0].shape[1]
    return pl.pallas_call(
        early_kernel,
        in_specs=[SMEM, ANY] + [HBM] * 8,
        out_specs=pl.BlockSpec((count, 3 * part), lambda: (0, 0)),
        scratch_shapes=[
            pltpu.VMEM((count, width), jnp.bfloat16),
            pltpu.VMEM((3, width, part), jnp.bfloat16),
            pltpu.VMEM((3, width, part), jnp.bfloat16),
            pltpu.SemaphoreType.DMA((7,)),
        ],
        out_shape=jax.ShapeDtypeStruct((count, 3 * part), jnp.bfloat16),
        compiler_params=pltpu.CompilerParams(vmem_limit_bytes=50 * MIB),
        name="early_hidden",
    )(place, rows, *gates, *ups)


def middle_hidden(place, rows, gates, ups):
    count, width = rows.shape
    part = gates[0].shape[1]
    return pl.pallas_call(
        middle_kernel,
        in_specs=[SMEM, ANY] + [HBM] * 4,
        out_specs=pl.BlockSpec((count, part), lambda: (0, 0)),
        scratch_shapes=[
            pltpu.VMEM((count, width), jnp.bfloat16),
            pltpu.VMEM((width, part), jnp.bfloat16),
            pltpu.VMEM((width, part), jnp.bfloat16),
            pltpu.SemaphoreType.DMA((3,)),
        ],
        out_shape=jax.ShapeDtypeStruct((count, part), jnp.bfloat16),
        compiler_params=pltpu.CompilerParams(vmem_limit_bytes=50 * MIB),
        name="middle_hidden",
    )(place, rows, *gates, *ups)


def late_kernel(place_ref, early_ref, middle_ref, d0a, d0b, d1, d2, d3a, d3b, out_ref, down, hidden, out, sems, out_sems):
    flag = place_ref[1]
    senders, pieces, slots, piece = out_ref.shape
    part = d1.shape[0]
    first = pltpu.make_async_copy(early_ref, hidden.at[:, pl.ds(0, 3 * part)], sems.at[4 * pieces])
    second = pltpu.make_async_copy(middle_ref, hidden.at[:, pl.ds(3 * part, part)], sems.at[4 * pieces + 1])
    first.start()
    second.start()

    def target(i, f):
        return down.at[pl.ds(i * part, part), pl.ds(f * piece, piece)]

    def source(ref, f):
        return ref.at[:, pl.ds(f * piece, piece)]

    for f in range(pieces):
        start_one(flag, source(d0a, f), source(d0b, f), target(0, f), sems.at[4 * f])
        pltpu.make_async_copy(source(d1, f), target(1, f), sems.at[4 * f + 1]).start()
        pltpu.make_async_copy(source(d2, f), target(2, f), sems.at[4 * f + 2]).start()
        start_one(flag, source(d3a, f), source(d3b, f), target(3, f), sems.at[4 * f + 3])
    first.wait()
    second.wait()
    for f in range(pieces):
        for i in range(4):
            pltpu.make_async_copy(source(d1, f), target(i, f), sems.at[4 * f + i]).wait()
        value = jnp.dot(
            hidden[...], down[:, f * piece : (f + 1) * piece], preferred_element_type=jnp.float32
        )
        out[f] = value.reshape(senders, slots, piece).astype(jnp.bfloat16)
        pltpu.make_async_copy(out.at[f], out_ref.at[:, f], out_sems.at[f]).start()
    for f in range(pieces):
        pltpu.make_async_copy(out.at[f], out_ref.at[:, f], out_sems.at[f]).wait()


def late_outputs(place, early, middle, downs, senders, pieces):
    count = early.shape[0]
    part, width = downs[0].shape
    slots = count // senders
    piece = width // pieces
    shape = (senders, pieces, slots, piece)
    return pl.pallas_call(
        late_kernel,
        in_specs=[SMEM, ANY, ANY] + [HBM] * 6,
        out_specs=HBM,
        scratch_shapes=[
            pltpu.VMEM((4 * part, width), jnp.bfloat16),
            pltpu.VMEM((count, 4 * part), jnp.bfloat16),
            pltpu.VMEM((pieces, senders, slots, piece), jnp.bfloat16),
            pltpu.SemaphoreType.DMA((4 * pieces + 2,)),
            pltpu.SemaphoreType.DMA((pieces,)),
        ],
        out_shape=pltpu.HBM(shape, jnp.bfloat16),
        compiler_params=pltpu.CompilerParams(vmem_limit_bytes=50 * MIB),
        name="late_outputs",
    )(place, early, middle, *downs)


def columns_kernel(ids_ref, out_ref, *, cuts, count_tp):
    count = ids_ref.shape[0]
    experts = 32
    first = ids_ref[:, 0:1]
    second = ids_ref[:, 1:2]
    number = lax.broadcasted_iota(jnp.int32, (count, experts), 1)
    named_first = number == first
    named_second = number == second
    named = jnp.where(named_first | named_second, 1.0, 0.0).astype(jnp.bfloat16)
    before = lax.broadcasted_iota(jnp.int32, (count, count), 1) < lax.broadcasted_iota(
        jnp.int32, (count, count), 0
    )
    ranks = jnp.dot(
        jnp.where(before, 1.0, 0.0).astype(jnp.bfloat16), named, preferred_element_type=jnp.float32
    )
    for choice, (ids, chosen) in enumerate(((first, named_first), (second, named_second))):
        slot = jnp.sum(jnp.where(chosen, ranks, 0.0), axis=1, keepdims=True).astype(jnp.int32)
        ep, tp, row = place_of(ids, slot)
        device = ep * count_tp + tp
        for i, (lo, hi) in enumerate(cuts):
            inside = (row >= lo) & (row < hi)
            out_ref[:, 2 * i + choice : 2 * i + choice + 1] = jnp.where(
                inside, device * (hi - lo) + row - lo, -1
            )


def routing_columns(ids, cuts, count_tp):
    return pl.pallas_call(
        functools.partial(columns_kernel, cuts=cuts, count_tp=count_tp),
        out_shape=jax.ShapeDtypeStruct((ids.shape[0], 2 * len(cuts)), jnp.int32),
        compiler_params=pltpu.CompilerParams(vmem_limit_bytes=16 * MIB),
        name="columns",
    )(ids)


def combine_kernel(index_ref, scores_ref, returned_ref, out_ref, squares_ref):
    total = returned_ref.shape[0]
    count = index_ref.shape[0]
    index = lax.broadcasted_iota(jnp.int32, (count, total), 1)
    returned = returned_ref[...]

    def picked(column):
        hot = jnp.where(index == index_ref[:, column : column + 1], 1.0, 0.0).astype(jnp.bfloat16)
        return jnp.dot(hot, returned, preferred_element_type=jnp.float32)

    scores = scores_ref[...]
    mix = scores / jnp.sum(scores, axis=1, keepdims=True)
    value = mix[:, 0:1] * picked(0) + mix[:, 1:2] * picked(1)
    out_ref[...] = value
    square = value * value
    lanes = 128
    folded = square[:, 0:lanes]
    for i in range(1, square.shape[1] // lanes):
        folded = folded + square[:, i * lanes : (i + 1) * lanes]
    squares_ref[...] = jnp.sum(folded.T, axis=0, keepdims=True)


def combine(index, scores, returned):
    count = index.shape[0]
    total, piece = returned.shape
    steps = 3
    block = count // steps
    row_block = pl.BlockSpec((block, piece), lambda i: (i, 0))
    return pl.pallas_call(
        combine_kernel,
        grid=(steps,),
        in_specs=[
            pl.BlockSpec((block, 2), lambda i: (i, 0)),
            pl.BlockSpec((block, 2), lambda i: (i, 0)),
            pl.BlockSpec((total, piece), lambda i: (0, 0)),
        ],
        out_specs=[row_block, pl.BlockSpec((1, block), lambda i: (0, i))],
        out_shape=[
            jax.ShapeDtypeStruct((count, piece), jnp.float32),
            jax.ShapeDtypeStruct((1, count), jnp.float32),
        ],
        compiler_params=pltpu.CompilerParams(dimension_semantics=("arbitrary",), vmem_limit_bytes=50 * MIB),
        name="combine",
    )(index, scores, returned)


def per_device(
    tokens, in_gain, route_ids, route_scores, gate_weight, up_weight, down_weight, out_gain
):
    count_ep = lax.axis_size("ep")
    count_tp = lax.axis_size("tp")
    tok_count, full_width = tokens.shape
    part_width = full_width // count_tp
    capacity = 2 * tok_count * route_ids.shape[1] // count_ep
    rows = capacity // count_tp
    x = lax.axis_index("tp")
    core = lax.axis_index("ep") % 2
    place = jnp.stack([x, (x // 2 == core).astype(jnp.int32)]).astype(jnp.int32)

    first, second, swap = permutes(count_ep, count_tp)

    def send(weight, pairs):
        return lax.ppermute(weight, AXES, pairs)

    def spread(weight):
        moved = send(weight, first)
        other_own = send(weight, swap)
        other_moved = send(moved, swap)
        last = send(moved, second)
        other_last = send(last, swap)
        return (weight, other_own), moved, other_moved, (other_last, last)

    gate = spread(gate_weight[0])
    up = spread(up_weight[0])
    down = spread(down_weight[0])

    buffer = dispatch_buffer(place, route_ids.T, in_gain[None, :], tokens, rows)
    received = lax.all_to_all(
        buffer.reshape(count_ep, rows, full_width), "ep", split_axis=0, concat_axis=0, tiled=True
    ).reshape(count_ep * rows, full_width)
    early = early_hidden(place, received, (*gate[0], gate[1], gate[2]), (*up[0], up[1], up[2]))
    middle = middle_hidden(place, received, gate[3], up[3])
    outputs = late_outputs(
        place, early, middle, (*down[0], down[1], down[2], *down[3]), count_ep, count_tp
    )
    returned = lax.all_to_all(
        outputs.reshape(count_ep * count_tp, rows, part_width), AXES, split_axis=0, concat_axis=0, tiled=True
    ).reshape(count_ep * count_tp * rows, part_width)
    index = routing_columns(route_ids, ((0, rows),), count_tp)
    combined, squares = combine(index, route_scores, returned)
    squares = squares[0]
    total = squares
    for shift in range(1, count_tp):
        total = total + lax.ppermute(
            squares, "tp", [(i, (i + shift) % count_tp) for i in range(count_tp)]
        )
    scaled = combined * lax.rsqrt(total[:, None] / full_width + epsilon) * out_gain
    return scaled.astype(jnp.bfloat16)


def solution(mesh):
    in_specs = (
        P("ep", None),
        P(),
        P("ep", None),
        P("ep", None),
        P("ep", None, "tp"),
        P("ep", None, "tp"),
        P("ep", "tp", None),
        P("tp"),
    )
    out_specs = P("ep", "tp")
    return jax.shard_map(per_device, mesh=mesh, in_specs=in_specs, out_specs=out_specs, check_vma=False)
```

```python
import functools

import jax
import jax.numpy as jnp
from jax import lax
from jax.experimental import pallas as pl
from jax.experimental.pallas import tpu as pltpu
from jax.sharding import PartitionSpec as P


epsilon = 1e-06
AXES = ("ep", "tp")
MIB = 1024 * 1024


def place_of(ids, slot):
    ep = (ids // 2) * 2 + slot % 2
    tp = (ids % 2) * 2 + (slot % 4) // 2
    return ep, tp, slot // 4


def permutes(count_ep, count_tp):
    def dev(ep, x):
        return ep * count_tp + x

    first, second, swap = [], [], []
    for ep in range(count_ep):
        core = ep % 2
        for x in range(count_tp):
            own = x // 2 == core
            swap.append((dev(ep, x), dev(ep ^ 1, x)))
            if own:
                first.append((dev(ep, x), dev(ep, x ^ 1)))
            else:
                first.append((dev(ep, x), dev(ep ^ 1, count_tp - 1 - x)))
                second.append((dev(ep, x), dev(ep, x ^ 1)))
    return first, second, swap


def dispatch_kernel(ids_ref, gain_ref, tokens_ref, out_ref, raw, pick, sems, *, rows, chunks):
    step = pl.program_id(0)
    count, _ = raw.shape
    part = count // chunks

    def load(i):
        return pltpu.make_async_copy(
            tokens_ref.at[pl.ds(i * part, part)], raw.at[pl.ds(i * part, part)], sems.at[i]
        )

    @pl.when(step == 0)
    def _():
        for i in range(chunks):
            load(i).start()
        experts = 32
        first = ids_ref[0:1, :]
        second = ids_ref[1:2, :]
        number = lax.broadcasted_iota(jnp.int32, (experts, count), 0)
        named_first = number == first
        named_second = number == second
        named = jnp.where(named_first | named_second, 1.0, 0.0).astype(jnp.bfloat16)
        before = lax.broadcasted_iota(jnp.int32, (count, count), 0) < lax.broadcasted_iota(
            jnp.int32, (count, count), 1
        )
        ranks = jnp.dot(
            named, jnp.where(before, 1.0, 0.0).astype(jnp.bfloat16), preferred_element_type=jnp.float32
        )
        slot_first = jnp.sum(jnp.where(named_first, ranks, 0.0), axis=0, keepdims=True).astype(jnp.int32)
        slot_second = jnp.sum(jnp.where(named_second, ranks, 0.0), axis=0, keepdims=True).astype(jnp.int32)
        mine = lax.axis_index("tp")

        def row_of(ids, slot):
            ep, tp, row = place_of(ids, slot)
            return jnp.where(tp == mine, ep * rows + row, -1)

        row_first = row_of(first, slot_first)
        row_second = row_of(second, slot_second)
        index = lax.broadcasted_iota(jnp.int32, (count, count), 0)
        pick[...] = jnp.where((index == row_first) | (index == row_second), 1.0, 0.0).astype(jnp.bfloat16)
        for i in range(chunks):
            load(i).wait()

    block = out_ref.shape[0]
    value = jnp.dot(pick[pl.ds(step * block, block), :], raw[...], preferred_element_type=jnp.float32)
    mean = jnp.mean(value * value, axis=1, keepdims=True)
    out_ref[...] = (value * lax.rsqrt(mean + epsilon) * gain_ref[...]).astype(jnp.bfloat16)


def dispatch_buffer(ids_rows, gain, tokens, rows):
    count, width = tokens.shape
    steps, chunks = 6, 2
    return pl.pallas_call(
        functools.partial(dispatch_kernel, rows=rows, chunks=chunks),
        grid=(steps,),
        in_specs=[
            pl.BlockSpec((2, count), lambda i: (0, 0)),
            pl.BlockSpec((1, width), lambda i: (0, 0)),
            pl.BlockSpec(memory_space=pltpu.HBM),
        ],
        out_specs=pl.BlockSpec((count // steps, width), lambda i: (i, 0)),
        scratch_shapes=[
            pltpu.VMEM((count, width), jnp.bfloat16),
            pltpu.VMEM((count, count), jnp.bfloat16),
            pltpu.SemaphoreType.DMA((chunks,)),
        ],
        out_shape=pltpu.HBM((count, width), jnp.bfloat16),
        compiler_params=pltpu.CompilerParams(dimension_semantics=("arbitrary",), vmem_limit_bytes=58 * MIB),
        name="dispatch_buffer",
    )(ids_rows, gain, tokens)


def start_one(flag, a, b, dst, sem):
    @pl.when(flag == 1)
    def _():
        pltpu.make_async_copy(a, dst, sem).start()

    @pl.when(flag != 1)
    def _():
        pltpu.make_async_copy(b, dst, sem).start()


def hidden_kernel(place_ref, rows_ref, *refs, pieces):
    gates, ups = refs[:6], refs[6:12]
    out_ref, rows, weights, sems = refs[12:]
    flag = place_ref[1]
    count = rows.shape[0]
    part = gates[0].shape[1]
    size = count // pieces

    def start(refs, i, lo, sem):
        dst = weights.at[i, :, pl.ds(lo, part)]
        if i == 0 or i == 3:
            at = 0 if i == 0 else 4
            start_one(flag, refs[at], refs[at + 1], dst, sem)
        else:
            pltpu.make_async_copy(refs[i + 1], dst, sem).start()

    def load(p):
        return pltpu.make_async_copy(
            rows_ref.at[pl.ds(p * size, size)], rows.at[pl.ds(p * size, size)], sems.at[8 + p]
        )

    for i in range(4):
        start(gates, i, 0, sems.at[2 * i])
        start(ups, i, part, sems.at[2 * i + 1])
        if i == 0:
            for p in range(pieces):
                load(p).start()
    for i in range(4):
        pltpu.make_async_copy(gates[2], weights.at[i, :, pl.ds(0, part)], sems.at[2 * i]).wait()
        pltpu.make_async_copy(ups[2], weights.at[i, :, pl.ds(part, part)], sems.at[2 * i + 1]).wait()
        for p in range(pieces):
            if i == 0:
                load(p).wait()
            acts = jnp.dot(
                rows[p * size : (p + 1) * size, :], weights[i], preferred_element_type=jnp.float32
            )
            gate_acts = acts[:, :part]
            value = gate_acts / (1.0 + jnp.exp(-gate_acts)) * acts[:, part:]
            out_ref[p * size : (p + 1) * size, i * part : (i + 1) * part] = value.astype(jnp.bfloat16)


HBM = pl.BlockSpec(memory_space=pltpu.HBM)
ANY = pl.BlockSpec(memory_space=pl.ANY)
SMEM = pl.BlockSpec(memory_space=pltpu.SMEM)


def hidden_units(place, rows, gates, ups):
    count, width = rows.shape
    part = gates[0].shape[1]
    pieces = 2
    return pl.pallas_call(
        functools.partial(hidden_kernel, pieces=pieces),
        in_specs=[SMEM, ANY] + [HBM] * 12,
        out_specs=pl.BlockSpec((count, 4 * part), lambda: (0, 0)),
        scratch_shapes=[
            pltpu.VMEM((count, width), jnp.bfloat16),
            pltpu.VMEM((4, width, 2 * part), jnp.bfloat16),
            pltpu.SemaphoreType.DMA((8 + pieces,)),
        ],
        out_shape=jax.ShapeDtypeStruct((count, 4 * part), jnp.bfloat16),
        compiler_params=pltpu.CompilerParams(vmem_limit_bytes=50 * MIB),
        name="hidden_units",
    )(place, rows, *gates, *ups)


def late_kernel(place_ref, hidden_ref, d0a, d0b, d1, d2, d3a, d3b, out_ref, down, hidden, out, sems, out_sems):
    flag = place_ref[1]
    senders, pieces, slots, piece = out_ref.shape
    part = d1.shape[0]
    load = pltpu.make_async_copy(hidden_ref, hidden, sems.at[4 * pieces])
    load.start()

    def target(i, f):
        return down.at[pl.ds(i * part, part), pl.ds(f * piece, piece)]

    def source(ref, f):
        return ref.at[:, pl.ds(f * piece, piece)]

    for f in range(pieces):
        start_one(flag, source(d0a, f), source(d0b, f), target(0, f), sems.at[4 * f])
        pltpu.make_async_copy(source(d1, f), target(1, f), sems.at[4 * f + 1]).start()
        pltpu.make_async_copy(source(d2, f), target(2, f), sems.at[4 * f + 2]).start()
        start_one(flag, source(d3a, f), source(d3b, f), target(3, f), sems.at[4 * f + 3])
    load.wait()
    for f in range(pieces):
        for i in range(4):
            pltpu.make_async_copy(source(d1, f), target(i, f), sems.at[4 * f + i]).wait()
        value = jnp.dot(
            hidden[...], down[:, f * piece : (f + 1) * piece], preferred_element_type=jnp.float32
        )
        out[f] = value.reshape(senders, slots, piece).astype(jnp.bfloat16)
        pltpu.make_async_copy(out.at[f], out_ref.at[:, f], out_sems.at[f]).start()
    for f in range(pieces):
        pltpu.make_async_copy(out.at[f], out_ref.at[:, f], out_sems.at[f]).wait()


def late_outputs(place, hidden, downs, senders, pieces):
    count = hidden.shape[0]
    part, width = downs[0].shape
    slots = count // senders
    piece = width // pieces
    shape = (senders, pieces, slots, piece)
    return pl.pallas_call(
        late_kernel,
        in_specs=[SMEM, ANY] + [HBM] * 6,
        out_specs=HBM,
        scratch_shapes=[
            pltpu.VMEM((4 * part, width), jnp.bfloat16),
            pltpu.VMEM((count, 4 * part), jnp.bfloat16),
            pltpu.VMEM((pieces, senders, slots, piece), jnp.bfloat16),
            pltpu.SemaphoreType.DMA((4 * pieces + 1,)),
            pltpu.SemaphoreType.DMA((pieces,)),
        ],
        out_shape=pltpu.HBM(shape, jnp.bfloat16),
        compiler_params=pltpu.CompilerParams(vmem_limit_bytes=50 * MIB),
        name="late_outputs",
    )(place, hidden, *downs)


def columns_kernel(ids_ref, out_ref, *, cuts, count_tp):
    count = ids_ref.shape[0]
    experts = 32
    first = ids_ref[:, 0:1]
    second = ids_ref[:, 1:2]
    number = lax.broadcasted_iota(jnp.int32, (count, experts), 1)
    named_first = number == first
    named_second = number == second
    named = jnp.where(named_first | named_second, 1.0, 0.0).astype(jnp.bfloat16)
    before = lax.broadcasted_iota(jnp.int32, (count, count), 1) < lax.broadcasted_iota(
        jnp.int32, (count, count), 0
    )
    ranks = jnp.dot(
        jnp.where(before, 1.0, 0.0).astype(jnp.bfloat16), named, preferred_element_type=jnp.float32
    )
    for choice, (ids, chosen) in enumerate(((first, named_first), (second, named_second))):
        slot = jnp.sum(jnp.where(chosen, ranks, 0.0), axis=1, keepdims=True).astype(jnp.int32)
        ep, tp, row = place_of(ids, slot)
        device = ep * count_tp + tp
        for i, (lo, hi) in enumerate(cuts):
            inside = (row >= lo) & (row < hi)
            out_ref[:, 2 * i + choice : 2 * i + choice + 1] = jnp.where(
                inside, device * (hi - lo) + row - lo, -1
            )


def routing_columns(ids, cuts, count_tp):
    return pl.pallas_call(
        functools.partial(columns_kernel, cuts=cuts, count_tp=count_tp),
        out_shape=jax.ShapeDtypeStruct((ids.shape[0], 2 * len(cuts)), jnp.int32),
        compiler_params=pltpu.CompilerParams(vmem_limit_bytes=16 * MIB),
        name="columns",
    )(ids)


def combine_kernel(index_ref, scores_ref, returned_ref, out_ref, squares_ref):
    total = returned_ref.shape[0]
    count = index_ref.shape[0]
    index = lax.broadcasted_iota(jnp.int32, (count, total), 1)
    returned = returned_ref[...]

    def picked(column):
        hot = jnp.where(index == index_ref[:, column : column + 1], 1.0, 0.0).astype(jnp.bfloat16)
        return jnp.dot(hot, returned, preferred_element_type=jnp.float32)

    scores = scores_ref[...]
    mix = scores / jnp.sum(scores, axis=1, keepdims=True)
    value = mix[:, 0:1] * picked(0) + mix[:, 1:2] * picked(1)
    out_ref[...] = value
    square = value * value
    lanes = 128
    folded = square[:, 0:lanes]
    for i in range(1, square.shape[1] // lanes):
        folded = folded + square[:, i * lanes : (i + 1) * lanes]
    squares_ref[...] = jnp.sum(folded.T, axis=0, keepdims=True)


def combine(index, scores, returned):
    count = index.shape[0]
    total, piece = returned.shape
    steps = 3
    block = count // steps
    row_block = pl.BlockSpec((block, piece), lambda i: (i, 0))
    return pl.pallas_call(
        combine_kernel,
        grid=(steps,),
        in_specs=[
            pl.BlockSpec((block, 2), lambda i: (i, 0)),
            pl.BlockSpec((block, 2), lambda i: (i, 0)),
            pl.BlockSpec((total, piece), lambda i: (0, 0)),
        ],
        out_specs=[row_block, pl.BlockSpec((1, block), lambda i: (0, i))],
        out_shape=[
            jax.ShapeDtypeStruct((count, piece), jnp.float32),
            jax.ShapeDtypeStruct((1, count), jnp.float32),
        ],
        compiler_params=pltpu.CompilerParams(dimension_semantics=("arbitrary",), vmem_limit_bytes=50 * MIB),
        name="combine",
    )(index, scores, returned)


def per_device(
    tokens, in_gain, route_ids, route_scores, gate_weight, up_weight, down_weight, out_gain
):
    count_ep = lax.axis_size("ep")
    count_tp = lax.axis_size("tp")
    tok_count, full_width = tokens.shape
    part_width = full_width // count_tp
    capacity = 2 * tok_count * route_ids.shape[1] // count_ep
    rows = capacity // count_tp
    x = lax.axis_index("tp")
    core = lax.axis_index("ep") % 2
    place = jnp.stack([x, (x // 2 == core).astype(jnp.int32)]).astype(jnp.int32)

    first, second, swap = permutes(count_ep, count_tp)

    def send(weight, pairs):
        return lax.ppermute(weight, AXES, pairs)

    def spread(weight):
        moved = send(weight, first)
        other_own = send(weight, swap)
        other_moved = send(moved, swap)
        last = send(moved, second)
        other_last = send(last, swap)
        return (weight, other_own), moved, other_moved, (other_last, last)

    gate = spread(gate_weight[0])
    up = spread(up_weight[0])
    down = spread(down_weight[0])

    buffer = dispatch_buffer(route_ids.T, in_gain[None, :], tokens, rows)
    received = lax.all_to_all(
        buffer.reshape(count_ep, rows, full_width), "ep", split_axis=0, concat_axis=0, tiled=True
    ).reshape(count_ep * rows, full_width)
    hidden = hidden_units(
        place, received, (*gate[0], gate[1], gate[2], *gate[3]), (*up[0], up[1], up[2], *up[3])
    )
    outputs = late_outputs(
        place, hidden, (*down[0], down[1], down[2], *down[3]), count_ep, count_tp
    )
    returned = lax.all_to_all(
        outputs.reshape(count_ep * count_tp, rows, part_width), AXES, split_axis=0, concat_axis=0, tiled=True
    ).reshape(count_ep * count_tp * rows, part_width)
    index = routing_columns(route_ids, ((0, rows),), count_tp)
    combined, squares = combine(index, route_scores, returned)
    squares = squares[0]
    total = squares
    for shift in range(1, count_tp):
        total = total + lax.ppermute(
            squares, "tp", [(i, (i + shift) % count_tp) for i in range(count_tp)]
        )
    scaled = combined * lax.rsqrt(total[:, None] / full_width + epsilon) * out_gain
    return scaled.astype(jnp.bfloat16)


def solution(mesh):
    in_specs = (
        P("ep", None),
        P(),
        P("ep", None),
        P("ep", None),
        P("ep", None, "tp"),
        P("ep", None, "tp"),
        P("ep", "tp", None),
        P("tp"),
    )
    out_specs = P("ep", "tp")
    return jax.shard_map(per_device, mesh=mesh, in_specs=in_specs, out_specs=out_specs, check_vma=False)
```

```python
import functools

import jax
import jax.numpy as jnp
from jax import lax
from jax.experimental import pallas as pl
from jax.experimental.pallas import tpu as pltpu
from jax.sharding import PartitionSpec as P


epsilon = 1e-06
AXES = ("ep", "tp")
MIB = 1024 * 1024


def place_of(ids, slot):
    ep = (ids // 2) * 2 + slot % 2
    tp = (ids % 2) * 2 + (slot % 4) // 2
    return ep, tp, slot // 4


def in_vmem(value):
    return pltpu.with_memory_space_constraint(value, pltpu.VMEM)


def in_hbm(value):
    return pltpu.with_memory_space_constraint(value, pltpu.HBM)


def permutes(count_ep, count_tp):
    def dev(ep, x):
        return ep * count_tp + x

    first, second, swap = [], [], []
    for ep in range(count_ep):
        core = ep % 2
        for x in range(count_tp):
            own = x // 2 == core
            swap.append((dev(ep, x), dev(ep ^ 1, x)))
            if own:
                first.append((dev(ep, x), dev(ep, x ^ 1)))
            else:
                first.append((dev(ep, x), dev(ep ^ 1, count_tp - 1 - x)))
                second.append((dev(ep, x), dev(ep, x ^ 1)))
    return first, second, swap


def dispatch_kernel(ids_ref, gain_ref, tokens_ref, out_ref, raw, pick, sems, *, rows, chunks):
    step = pl.program_id(0)
    count, _ = raw.shape
    part = count // chunks

    def load(i):
        return pltpu.make_async_copy(
            tokens_ref.at[pl.ds(i * part, part)], raw.at[pl.ds(i * part, part)], sems.at[i]
        )

    @pl.when(step == 0)
    def _():
        for i in range(chunks):
            load(i).start()
        experts = 32
        first = ids_ref[0:1, :]
        second = ids_ref[1:2, :]
        number = lax.broadcasted_iota(jnp.int32, (experts, count), 0)
        named_first = number == first
        named_second = number == second
        named = jnp.where(named_first | named_second, 1.0, 0.0).astype(jnp.bfloat16)
        before = lax.broadcasted_iota(jnp.int32, (count, count), 0) < lax.broadcasted_iota(
            jnp.int32, (count, count), 1
        )
        ranks = jnp.dot(
            named, jnp.where(before, 1.0, 0.0).astype(jnp.bfloat16), preferred_element_type=jnp.float32
        )
        slot_first = jnp.sum(jnp.where(named_first, ranks, 0.0), axis=0, keepdims=True).astype(jnp.int32)
        slot_second = jnp.sum(jnp.where(named_second, ranks, 0.0), axis=0, keepdims=True).astype(jnp.int32)
        mine = lax.axis_index("tp")

        def row_of(ids, slot):
            ep, tp, row = place_of(ids, slot)
            return jnp.where(tp == mine, ep * rows + row, -1)

        row_first = row_of(first, slot_first)
        row_second = row_of(second, slot_second)
        index = lax.broadcasted_iota(jnp.int32, (count, count), 0)
        pick[...] = jnp.where((index == row_first) | (index == row_second), 1.0, 0.0).astype(jnp.bfloat16)
        for i in range(chunks):
            load(i).wait()

    block = out_ref.shape[0]
    value = jnp.dot(pick[pl.ds(step * block, block), :], raw[...], preferred_element_type=jnp.float32)
    mean = jnp.mean(value * value, axis=1, keepdims=True)
    out_ref[...] = (value * lax.rsqrt(mean + epsilon) * gain_ref[...]).astype(jnp.bfloat16)


def dispatch_buffer(ids_rows, gain, tokens, rows):
    count, width = tokens.shape
    steps, chunks = 2, 2
    return pl.pallas_call(
        functools.partial(dispatch_kernel, rows=rows, chunks=chunks),
        grid=(steps,),
        in_specs=[
            pl.BlockSpec((2, count), lambda i: (0, 0)),
            pl.BlockSpec((1, width), lambda i: (0, 0)),
            pl.BlockSpec(memory_space=pltpu.HBM),
        ],
        out_specs=pl.BlockSpec((count // steps, width), lambda i: (i, 0)),
        scratch_shapes=[
            pltpu.VMEM((count, width), jnp.bfloat16),
            pltpu.VMEM((count, count), jnp.bfloat16),
            pltpu.SemaphoreType.DMA((chunks,)),
        ],
        out_shape=pltpu.HBM((count, width), jnp.bfloat16),
        compiler_params=pltpu.CompilerParams(dimension_semantics=("arbitrary",), vmem_limit_bytes=58 * MIB),
        name="dispatch_buffer",
    )(ids_rows, gain, tokens)


def start_one(flag, a, b, dst, sem):
    @pl.when(flag == 1)
    def _():
        pltpu.make_async_copy(a, dst, sem).start()

    @pl.when(flag != 1)
    def _():
        pltpu.make_async_copy(b, dst, sem).start()


def activation(acts, part):
    gate_acts = acts[:, :part]
    return (gate_acts / (1.0 + jnp.exp(-gate_acts)) * acts[:, part:]).astype(jnp.bfloat16)


def early_kernel(place_ref, rows_ref, *refs):
    gates, ups = refs[:4], refs[4:8]
    out_ref, weights, sems = refs[8:]
    flag = place_ref[1]
    part = gates[0].shape[1]
    for i in range(3):
        for lo, r, sem in ((0, gates, sems.at[2 * i]), (part, ups, sems.at[2 * i + 1])):
            dst = weights.at[i, :, pl.ds(lo, part)]
            if i == 0:
                start_one(flag, r[0], r[1], dst, sem)
            else:
                pltpu.make_async_copy(r[i + 1], dst, sem).start()
    for i in range(3):
        pltpu.make_async_copy(gates[2], weights.at[i, :, pl.ds(0, part)], sems.at[2 * i]).wait()
        pltpu.make_async_copy(ups[2], weights.at[i, :, pl.ds(part, part)], sems.at[2 * i + 1]).wait()
        acts = jnp.dot(rows_ref[...], weights[i], preferred_element_type=jnp.float32)
        out_ref[:, i * part : (i + 1) * part] = activation(acts, part)


def middle_kernel(place_ref, rows_ref, ga, gb, ua, ub, out_ref, weights, sems):
    flag = place_ref[1]
    part = ga.shape[1]
    start_one(flag, ga, gb, weights.at[:, pl.ds(0, part)], sems.at[0])
    start_one(flag, ua, ub, weights.at[:, pl.ds(part, part)], sems.at[1])
    pltpu.make_async_copy(ga, weights.at[:, pl.ds(0, part)], sems.at[0]).wait()
    pltpu.make_async_copy(ua, weights.at[:, pl.ds(part, part)], sems.at[1]).wait()
    acts = jnp.dot(rows_ref[...], weights[...], preferred_element_type=jnp.float32)
    out_ref[...] = activation(acts, part)


HBM = pl.BlockSpec(memory_space=pltpu.HBM)
ANY = pl.BlockSpec(memory_space=pl.ANY)
SMEM = pl.BlockSpec(memory_space=pltpu.SMEM)
VMEM = pl.BlockSpec(memory_space=pltpu.VMEM)


def early_hidden(place, rows, gates, ups):
    count, width = rows.shape
    part = gates[0].shape[1]
    return pl.pallas_call(
        early_kernel,
        in_specs=[SMEM, VMEM] + [ANY] * 8,
        out_specs=VMEM,
        scratch_shapes=[pltpu.VMEM((3, width, 2 * part), jnp.bfloat16), pltpu.SemaphoreType.DMA((6,))],
        out_shape=jax.ShapeDtypeStruct((count, 3 * part), jnp.bfloat16),
        compiler_params=pltpu.CompilerParams(vmem_limit_bytes=50 * MIB),
        name="early_hidden",
    )(place, rows, *gates, *ups)


def middle_hidden(place, rows, gates, ups):
    count, width = rows.shape
    part = gates[0].shape[1]
    return pl.pallas_call(
        middle_kernel,
        in_specs=[SMEM, VMEM] + [ANY] * 4,
        out_specs=VMEM,
        scratch_shapes=[pltpu.VMEM((width, 2 * part), jnp.bfloat16), pltpu.SemaphoreType.DMA((2,))],
        out_shape=jax.ShapeDtypeStruct((count, part), jnp.bfloat16),
        compiler_params=pltpu.CompilerParams(vmem_limit_bytes=50 * MIB),
        name="middle_hidden",
    )(place, rows, *gates, *ups)


def late_kernel(place_ref, early_ref, middle_ref, d0a, d0b, d1, d2, d3a, d3b, out_ref, down, hidden, out, sems, out_sems):
    flag = place_ref[1]
    senders, pieces, slots, piece = out_ref.shape
    part = d1.shape[0]

    def target(i, f):
        return down.at[pl.ds(i * part, part), pl.ds(f * piece, piece)]

    def source(ref, f):
        return ref.at[:, pl.ds(f * piece, piece)]

    for f in range(pieces):
        start_one(flag, source(d0a, f), source(d0b, f), target(0, f), sems.at[4 * f])
        pltpu.make_async_copy(source(d1, f), target(1, f), sems.at[4 * f + 1]).start()
        pltpu.make_async_copy(source(d2, f), target(2, f), sems.at[4 * f + 2]).start()
        start_one(flag, source(d3a, f), source(d3b, f), target(3, f), sems.at[4 * f + 3])
    hidden[:, 0 : 3 * part] = early_ref[...]
    hidden[:, 3 * part : 4 * part] = middle_ref[...]
    for f in range(pieces):
        for i in range(4):
            pltpu.make_async_copy(source(d1, f), target(i, f), sems.at[4 * f + i]).wait()
        value = jnp.dot(
            hidden[...], down[:, f * piece : (f + 1) * piece], preferred_element_type=jnp.float32
        )
        out[f] = value.reshape(senders, slots, piece).astype(jnp.bfloat16)
        pltpu.make_async_copy(out.at[f], out_ref.at[:, f], out_sems.at[f]).start()
    for f in range(pieces):
        pltpu.make_async_copy(out.at[f], out_ref.at[:, f], out_sems.at[f]).wait()


def late_outputs(place, early, middle, downs, senders, pieces):
    count = early.shape[0]
    part, width = downs[0].shape
    slots = count // senders
    piece = width // pieces
    shape = (senders, pieces, slots, piece)
    return pl.pallas_call(
        late_kernel,
        in_specs=[SMEM, VMEM, VMEM] + [ANY] * 6,
        out_specs=HBM,
        scratch_shapes=[
            pltpu.VMEM((4 * part, width), jnp.bfloat16),
            pltpu.VMEM((count, 4 * part), jnp.bfloat16),
            pltpu.VMEM((pieces, senders, slots, piece), jnp.bfloat16),
            pltpu.SemaphoreType.DMA((4 * pieces,)),
            pltpu.SemaphoreType.DMA((pieces,)),
        ],
        out_shape=pltpu.HBM(shape, jnp.bfloat16),
        compiler_params=pltpu.CompilerParams(vmem_limit_bytes=50 * MIB),
        name="late_outputs",
    )(place, early, middle, *downs)


def table_kernel(ids_ref, scores_ref, out_ref, *, rows, count_tp):
    count = ids_ref.shape[0]
    experts = 32
    first = ids_ref[:, 0:1]
    second = ids_ref[:, 1:2]
    number = lax.broadcasted_iota(jnp.int32, (count, experts), 1)
    named_first = number == first
    named_second = number == second
    named = jnp.where(named_first | named_second, 1.0, 0.0).astype(jnp.bfloat16)
    before = lax.broadcasted_iota(jnp.int32, (count, count), 1) < lax.broadcasted_iota(
        jnp.int32, (count, count), 0
    )
    ranks = jnp.dot(
        jnp.where(before, 1.0, 0.0).astype(jnp.bfloat16), named, preferred_element_type=jnp.float32
    )
    scores = scores_ref[...]
    out_ref[:, 2:4] = scores / jnp.sum(scores, axis=1, keepdims=True)
    for choice, (ids, chosen) in enumerate(((first, named_first), (second, named_second))):
        slot = jnp.sum(jnp.where(chosen, ranks, 0.0), axis=1, keepdims=True).astype(jnp.int32)
        ep, tp, row = place_of(ids, slot)
        out_ref[:, choice : choice + 1] = ((ep * count_tp + tp) * rows + row).astype(jnp.float32)


def routing_table(ids, scores, rows, count_tp):
    return pl.pallas_call(
        functools.partial(table_kernel, rows=rows, count_tp=count_tp),
        out_shape=jax.ShapeDtypeStruct((ids.shape[0], 4), jnp.float32),
        compiler_params=pltpu.CompilerParams(vmem_limit_bytes=16 * MIB),
        name="columns",
    )(ids, scores)


def combine_kernel(table_ref, returned_ref, out_ref, squares_ref):
    total = returned_ref.shape[0]
    count = table_ref.shape[0]
    index = lax.broadcasted_iota(jnp.int32, (count, total), 1)
    returned = returned_ref[...]

    def picked(choice):
        row = table_ref[:, choice : choice + 1].astype(jnp.int32)
        hot = jnp.where(index == row, 1.0, 0.0).astype(jnp.bfloat16)
        return jnp.dot(hot, returned, preferred_element_type=jnp.float32)

    value = table_ref[:, 2:3] * picked(0) + table_ref[:, 3:4] * picked(1)
    out_ref[...] = value
    square = value * value
    lanes = 128
    folded = square[:, 0:lanes]
    for i in range(1, square.shape[1] // lanes):
        folded = folded + square[:, i * lanes : (i + 1) * lanes]
    squares_ref[...] = jnp.sum(folded.T, axis=0, keepdims=True)


def combine(table, returned):
    count = table.shape[0]
    piece = returned.shape[1]
    return pl.pallas_call(
        combine_kernel,
        in_specs=[VMEM, VMEM],
        out_specs=[VMEM, VMEM],
        out_shape=[
            jax.ShapeDtypeStruct((count, piece), jnp.float32),
            jax.ShapeDtypeStruct((1, count), jnp.float32),
        ],
        compiler_params=pltpu.CompilerParams(vmem_limit_bytes=50 * MIB),
        name="combine",
    )(table, returned)


def per_device(
    tokens, in_gain, route_ids, route_scores, gate_weight, up_weight, down_weight, out_gain
):
    count_ep = lax.axis_size("ep")
    count_tp = lax.axis_size("tp")
    tok_count, full_width = tokens.shape
    part_width = full_width // count_tp
    capacity = 2 * tok_count * route_ids.shape[1] // count_ep
    rows = capacity // count_tp
    x = lax.axis_index("tp")
    core = lax.axis_index("ep") % 2
    place = jnp.stack([x, (x // 2 == core).astype(jnp.int32)]).astype(jnp.int32)

    first, second, swap = permutes(count_ep, count_tp)

    def send(weight, pairs):
        return lax.ppermute(weight, AXES, pairs)

    def spread(name, weight):
        moved = send(weight, first)
        other_own = send(weight, swap)
        other_moved = send(moved, swap)
        last = send(moved, second)
        other_last = send(last, swap)
        hold = in_vmem if name == "down" else in_hbm
        return (in_hbm(weight), in_hbm(other_own)), in_hbm(moved), in_hbm(other_moved), (hold(other_last), in_hbm(last))

    gate = spread("gate", gate_weight[0])
    up = spread("up", up_weight[0])
    down = spread("down", down_weight[0])

    buffer = dispatch_buffer(route_ids.T, in_gain[None, :], tokens, rows)
    received = lax.all_to_all(
        buffer.reshape(count_ep, rows, full_width), "ep", split_axis=0, concat_axis=0, tiled=True
    ).reshape(count_ep * rows, full_width)
    received = in_vmem(received)
    early = in_vmem(early_hidden(place, received, (*gate[0], gate[1], gate[2]), (*up[0], up[1], up[2])))
    middle = in_vmem(middle_hidden(place, received, gate[3], up[3]))
    outputs = late_outputs(
        place, early, middle, (*down[0], down[1], down[2], *down[3]), count_ep, count_tp
    )
    returned = lax.all_to_all(
        outputs.reshape(count_ep * count_tp, rows, part_width), AXES, split_axis=0, concat_axis=0, tiled=True
    ).reshape(count_ep * count_tp * rows, part_width)
    table = routing_table(route_ids, route_scores, rows, count_tp)
    combined, squares = combine(table, in_vmem(returned))
    squares = squares[0]
    total = squares
    for shift in range(1, count_tp):
        total = total + lax.ppermute(
            squares, "tp", [(i, (i + shift) % count_tp) for i in range(count_tp)]
        )
    scaled = combined * lax.rsqrt(total[:, None] / full_width + epsilon) * out_gain
    return scaled.astype(jnp.bfloat16)


def solution(mesh):
    in_specs = (
        P("ep", None),
        P(),
        P("ep", None),
        P("ep", None),
        P("ep", None, "tp"),
        P("ep", None, "tp"),
        P("ep", "tp", None),
        P("tp"),
    )
    out_specs = P("ep", "tp")
    return jax.shard_map(per_device, mesh=mesh, in_specs=in_specs, out_specs=out_specs, check_vma=False)
```

```python
import functools

import jax
import jax.numpy as jnp
from jax import lax
from jax.experimental import pallas as pl
from jax.experimental.pallas import tpu as pltpu
from jax.sharding import PartitionSpec as P


epsilon = 1e-06
AXES = ("ep", "tp")
MIB = 1024 * 1024


def place_of(ids, slot):
    ep = (ids // 2) * 2 + slot % 2
    tp = (ids % 2) * 2 + (slot % 4) // 2
    return ep, tp, slot // 4


def in_vmem(value):
    return pltpu.with_memory_space_constraint(value, pltpu.VMEM)


def in_hbm(value):
    return pltpu.with_memory_space_constraint(value, pltpu.HBM)


def permutes(count_ep, count_tp):
    def dev(ep, x):
        return ep * count_tp + x

    first, second, swap = [], [], []
    for ep in range(count_ep):
        core = ep % 2
        for x in range(count_tp):
            own = x // 2 == core
            swap.append((dev(ep, x), dev(ep ^ 1, x)))
            if own:
                first.append((dev(ep, x), dev(ep, x ^ 1)))
            else:
                first.append((dev(ep, x), dev(ep ^ 1, count_tp - 1 - x)))
                second.append((dev(ep, x), dev(ep, x ^ 1)))
    return first, second, swap


def dispatch_kernel(ids_ref, gain_ref, tokens_ref, out_ref, raw, pick, sems, *, rows, chunks):
    step = pl.program_id(0)
    count, _ = raw.shape
    part = count // chunks

    def load(i):
        return pltpu.make_async_copy(
            tokens_ref.at[pl.ds(i * part, part)], raw.at[pl.ds(i * part, part)], sems.at[i]
        )

    @pl.when(step == 0)
    def _():
        for i in range(chunks):
            load(i).start()
        experts = 32
        first = ids_ref[0:1, :]
        second = ids_ref[1:2, :]
        number = lax.broadcasted_iota(jnp.int32, (experts, count), 0)
        named_first = number == first
        named_second = number == second
        named = jnp.where(named_first | named_second, 1.0, 0.0).astype(jnp.bfloat16)
        before = lax.broadcasted_iota(jnp.int32, (count, count), 0) < lax.broadcasted_iota(
            jnp.int32, (count, count), 1
        )
        ranks = jnp.dot(
            named, jnp.where(before, 1.0, 0.0).astype(jnp.bfloat16), preferred_element_type=jnp.float32
        )
        slot_first = jnp.sum(jnp.where(named_first, ranks, 0.0), axis=0, keepdims=True).astype(jnp.int32)
        slot_second = jnp.sum(jnp.where(named_second, ranks, 0.0), axis=0, keepdims=True).astype(jnp.int32)
        mine = lax.axis_index("tp")

        def row_of(ids, slot):
            ep, tp, row = place_of(ids, slot)
            return jnp.where(tp == mine, ep * rows + row, -1)

        row_first = row_of(first, slot_first)
        row_second = row_of(second, slot_second)
        index = lax.broadcasted_iota(jnp.int32, (count, count), 0)
        pick[...] = jnp.where((index == row_first) | (index == row_second), 1.0, 0.0).astype(jnp.bfloat16)
        for i in range(chunks):
            load(i).wait()

    block = out_ref.shape[0]
    value = jnp.dot(pick[pl.ds(step * block, block), :], raw[...], preferred_element_type=jnp.float32)
    mean = jnp.mean(value * value, axis=1, keepdims=True)
    out_ref[...] = (value * lax.rsqrt(mean + epsilon) * gain_ref[...]).astype(jnp.bfloat16)


def dispatch_buffer(ids_rows, gain, tokens, rows):
    count, width = tokens.shape
    steps, chunks = 2, 2
    return pl.pallas_call(
        functools.partial(dispatch_kernel, rows=rows, chunks=chunks),
        grid=(steps,),
        in_specs=[
            pl.BlockSpec((2, count), lambda i: (0, 0)),
            pl.BlockSpec((1, width), lambda i: (0, 0)),
            pl.BlockSpec(memory_space=pltpu.HBM),
        ],
        out_specs=pl.BlockSpec((count // steps, width), lambda i: (i, 0)),
        scratch_shapes=[
            pltpu.VMEM((count, width), jnp.bfloat16),
            pltpu.VMEM((count, count), jnp.bfloat16),
            pltpu.SemaphoreType.DMA((chunks,)),
        ],
        out_shape=pltpu.HBM((count, width), jnp.bfloat16),
        compiler_params=pltpu.CompilerParams(dimension_semantics=("arbitrary",), vmem_limit_bytes=58 * MIB),
        name="dispatch_buffer",
    )(ids_rows, gain, tokens)


def start_one(flag, a, b, dst, sem):
    @pl.when(flag == 1)
    def _():
        pltpu.make_async_copy(a, dst, sem).start()

    @pl.when(flag != 1)
    def _():
        pltpu.make_async_copy(b, dst, sem).start()


def activation(acts, part):
    gate_acts = acts[:, :part]
    return (gate_acts / (1.0 + jnp.exp(-gate_acts)) * acts[:, part:]).astype(jnp.bfloat16)


def halves_of(width):
    return ((0, width // 2), (width // 2, width // 2))


def split_block(rows_ref, weights, waits):
    acts = None
    for (lo, size), wait in zip(halves_of(rows_ref.shape[1]), waits):
        wait()
        term = jnp.dot(
            rows_ref[:, lo : lo + size], weights[lo : lo + size, :], preferred_element_type=jnp.float32
        )
        acts = term if acts is None else acts + term
    return acts


def early_kernel(place_ref, rows_ref, ga, gb, g1, g2, ua, ub, u1, u2, out_ref, weights, sems):
    flag = place_ref[1]
    width, part = g1.shape

    def plain(at, lo, size, gate, up):
        for n, source in enumerate((gate, up)):
            yield (
                source.at[pl.ds(lo, size)],
                weights.at[at, pl.ds(lo, size), pl.ds(n * part, part)],
            )

    def wait_for(at, lo, size, sem):
        for n, (source, target) in enumerate(plain(at, lo, size, g1, u1)):
            pltpu.make_async_copy(source, target, sems.at[sem + n]).wait()

    for half, (lo, size) in enumerate(halves_of(width)):
        for n, (source, target) in enumerate(plain(0, lo, size, g1, u1)):
            pltpu.make_async_copy(source, target, sems.at[2 * half + n]).start()
    for n, (source, target) in enumerate(plain(1, 0, width, g2, u2)):
        pltpu.make_async_copy(source, target, sems.at[4 + n]).start()
    start_one(flag, ga, gb, weights.at[2, :, pl.ds(0, part)], sems.at[6])
    start_one(flag, ua, ub, weights.at[2, :, pl.ds(part, part)], sems.at[7])
    waits = [
        functools.partial(wait_for, 0, lo, size, 2 * half) for half, (lo, size) in enumerate(halves_of(width))
    ]
    out_ref[:, part : 2 * part] = activation(split_block(rows_ref, weights.at[0], waits), part)
    for at, out in ((1, 2), (2, 0)):
        wait_for(at, 0, width, 2 + 2 * at)
        acts = jnp.dot(rows_ref[...], weights[at], preferred_element_type=jnp.float32)
        out_ref[:, out * part : (out + 1) * part] = activation(acts, part)


def middle_kernel(place_ref, rows_ref, ga, gb, ua, ub, out_ref, weights, sems):
    flag = place_ref[1]
    width, part = ga.shape

    def target(lo, size, n):
        return weights.at[pl.ds(lo, size), pl.ds(n * part, part)]

    def wait_for(half, lo, size):
        for n in range(2):
            pltpu.make_async_copy(ga.at[pl.ds(lo, size)], target(lo, size, n), sems.at[2 * half + n]).wait()

    waits = []
    for half, (lo, size) in enumerate(halves_of(width)):
        for n, (a, b) in enumerate(((ga, gb), (ua, ub))):
            start_one(flag, a.at[pl.ds(lo, size)], b.at[pl.ds(lo, size)], target(lo, size, n), sems.at[2 * half + n])
        waits.append(functools.partial(wait_for, half, lo, size))
    out_ref[...] = activation(split_block(rows_ref, weights, waits), part)


HBM = pl.BlockSpec(memory_space=pltpu.HBM)
ANY = pl.BlockSpec(memory_space=pl.ANY)
SMEM = pl.BlockSpec(memory_space=pltpu.SMEM)
VMEM = pl.BlockSpec(memory_space=pltpu.VMEM)


def early_hidden(place, rows, gates, ups):
    count, width = rows.shape
    part = gates[0].shape[1]
    return pl.pallas_call(
        early_kernel,
        in_specs=[SMEM, VMEM] + [ANY] * 8,
        out_specs=VMEM,
        scratch_shapes=[pltpu.VMEM((3, width, 2 * part), jnp.bfloat16), pltpu.SemaphoreType.DMA((8,))],
        out_shape=pltpu.VMEM((count, 3 * part), jnp.bfloat16),
        compiler_params=pltpu.CompilerParams(vmem_limit_bytes=50 * MIB),
        name="early_hidden",
    )(place, rows, *gates, *ups)


def middle_hidden(place, rows, gates, ups):
    count, width = rows.shape
    part = gates[0].shape[1]
    return pl.pallas_call(
        middle_kernel,
        in_specs=[SMEM, VMEM] + [ANY] * 4,
        out_specs=VMEM,
        scratch_shapes=[pltpu.VMEM((width, 2 * part), jnp.bfloat16), pltpu.SemaphoreType.DMA((4,))],
        out_shape=jax.ShapeDtypeStruct((count, part), jnp.bfloat16),
        compiler_params=pltpu.CompilerParams(vmem_limit_bytes=50 * MIB),
        name="middle_hidden",
    )(place, rows, *gates, *ups)


def late_kernel(place_ref, early_ref, middle_ref, d0a, d0b, d1, d2, d3a, d3b, out_ref, down, hidden, out, sems, out_sems, *, cuts):
    flag = place_ref[1]
    senders, pieces, slots, piece = out_ref.shape
    part = d1.shape[0]
    size = piece // cuts
    steps = pieces * cuts

    def target(i, f):
        return down.at[pl.ds(i * part, part), pl.ds(f * size, size)]

    def source(ref, f):
        return ref.at[:, pl.ds(f * size, size)]

    for f in range(steps):
        pltpu.make_async_copy(source(d1, f), target(1, f), sems.at[4 * f + 1]).start()
        pltpu.make_async_copy(source(d2, f), target(2, f), sems.at[4 * f + 2]).start()
        start_one(flag, source(d0a, f), source(d0b, f), target(0, f), sems.at[4 * f])
        start_one(flag, source(d3a, f), source(d3b, f), target(3, f), sems.at[4 * f + 3])
    hidden[:, 0 : 3 * part] = early_ref[...]
    hidden[:, 3 * part : 4 * part] = middle_ref[...]

    def store(f):
        return pltpu.make_async_copy(
            out.at[f], out_ref.at[:, f // cuts, :, pl.ds(f % cuts * size, size)], out_sems.at[f]
        )

    for f in range(steps):
        for i in range(4):
            pltpu.make_async_copy(source(d1, f), target(i, f), sems.at[4 * f + i]).wait()
        value = jnp.dot(
            hidden[...], down[:, f * size : (f + 1) * size], preferred_element_type=jnp.float32
        )
        out[f] = value.reshape(senders, slots, size).astype(jnp.bfloat16)
        store(f).start()
    for f in range(steps):
        store(f).wait()


def late_outputs(place, early, middle, downs, senders, pieces):
    count = early.shape[0]
    part, width = downs[0].shape
    slots = count // senders
    piece = width // pieces
    shape = (senders, pieces, slots, piece)
    cuts = 2
    return pl.pallas_call(
        functools.partial(late_kernel, cuts=cuts),
        in_specs=[SMEM, VMEM, VMEM] + [ANY] * 6,
        out_specs=HBM,
        scratch_shapes=[
            pltpu.VMEM((4 * part, width), jnp.bfloat16),
            pltpu.VMEM((count, 4 * part), jnp.bfloat16),
            pltpu.VMEM((pieces * cuts, senders, slots, piece // cuts), jnp.bfloat16),
            pltpu.SemaphoreType.DMA((4 * pieces * cuts,)),
            pltpu.SemaphoreType.DMA((pieces * cuts,)),
        ],
        out_shape=pltpu.HBM(shape, jnp.bfloat16),
        compiler_params=pltpu.CompilerParams(vmem_limit_bytes=50 * MIB),
        name="late_outputs",
    )(place, early, middle, *downs)


def table_kernel(ids_ref, scores_ref, out_ref, *, rows, count_tp):
    count = ids_ref.shape[0]
    experts = 32
    first = ids_ref[:, 0:1]
    second = ids_ref[:, 1:2]
    number = lax.broadcasted_iota(jnp.int32, (count, experts), 1)
    named_first = number == first
    named_second = number == second
    named = jnp.where(named_first | named_second, 1.0, 0.0).astype(jnp.bfloat16)
    before = lax.broadcasted_iota(jnp.int32, (count, count), 1) < lax.broadcasted_iota(
        jnp.int32, (count, count), 0
    )
    ranks = jnp.dot(
        jnp.where(before, 1.0, 0.0).astype(jnp.bfloat16), named, preferred_element_type=jnp.float32
    )
    scores = scores_ref[...]
    out_ref[:, 2:4] = scores / jnp.sum(scores, axis=1, keepdims=True)
    for choice, (ids, chosen) in enumerate(((first, named_first), (second, named_second))):
        slot = jnp.sum(jnp.where(chosen, ranks, 0.0), axis=1, keepdims=True).astype(jnp.int32)
        ep, tp, row = place_of(ids, slot)
        out_ref[:, choice : choice + 1] = ((ep * count_tp + tp) * rows + row).astype(jnp.float32)


def routing_table(ids, scores, rows, count_tp):
    return pl.pallas_call(
        functools.partial(table_kernel, rows=rows, count_tp=count_tp),
        out_shape=jax.ShapeDtypeStruct((ids.shape[0], 4), jnp.float32),
        compiler_params=pltpu.CompilerParams(vmem_limit_bytes=16 * MIB),
        name="columns",
    )(ids, scores)


def combine_kernel(table_ref, returned_ref, out_ref, squares_ref):
    total = returned_ref.shape[0]
    count = table_ref.shape[0]
    index = lax.broadcasted_iota(jnp.int32, (count, total), 1)
    returned = returned_ref[...]

    def picked(choice):
        row = table_ref[:, choice : choice + 1].astype(jnp.int32)
        hot = jnp.where(index == row, 1.0, 0.0).astype(jnp.bfloat16)
        return jnp.dot(hot, returned, preferred_element_type=jnp.float32)

    value = table_ref[:, 2:3] * picked(0) + table_ref[:, 3:4] * picked(1)
    out_ref[...] = value
    square = value * value
    lanes = 128
    folded = square[:, 0:lanes]
    for i in range(1, square.shape[1] // lanes):
        folded = folded + square[:, i * lanes : (i + 1) * lanes]
    squares_ref[...] = jnp.sum(folded.T, axis=0, keepdims=True)


def combine(table, returned):
    count = table.shape[0]
    piece = returned.shape[1]
    return pl.pallas_call(
        combine_kernel,
        in_specs=[VMEM, VMEM],
        out_specs=[VMEM, VMEM],
        out_shape=[
            pltpu.VMEM((count, piece), jnp.float32),
            jax.ShapeDtypeStruct((1, count), jnp.float32),
        ],
        compiler_params=pltpu.CompilerParams(vmem_limit_bytes=32 * MIB),
        name="combine",
    )(table, returned)


def scale_kernel(combined_ref, own_ref, a_ref, b_ref, c_ref, gain_ref, out_ref, *, width):
    total = own_ref[...] + a_ref[...] + b_ref[...] + c_ref[...]
    factor = lax.rsqrt(total / width + epsilon)
    count, piece = combined_ref.shape
    lanes = 128
    column = jnp.broadcast_to(factor, (lanes, count)).T
    for i in range(piece // lanes):
        at = slice(i * lanes, (i + 1) * lanes)
        out_ref[:, at] = (combined_ref[:, at] * column * gain_ref[:, at]).astype(jnp.bfloat16)


def scale(combined, squares, gain, width):
    count, piece = combined.shape
    return pl.pallas_call(
        functools.partial(scale_kernel, width=width),
        in_specs=[VMEM] * 6,
        out_specs=VMEM,
        out_shape=jax.ShapeDtypeStruct((count, piece), jnp.bfloat16),
        compiler_params=pltpu.CompilerParams(vmem_limit_bytes=16 * MIB),
        name="scale",
    )(combined, *squares, gain)


def per_device(
    tokens, in_gain, route_ids, route_scores, gate_weight, up_weight, down_weight, out_gain
):
    count_ep = lax.axis_size("ep")
    count_tp = lax.axis_size("tp")
    tok_count, full_width = tokens.shape
    part_width = full_width // count_tp
    capacity = 2 * tok_count * route_ids.shape[1] // count_ep
    rows = capacity // count_tp
    x = lax.axis_index("tp")
    core = lax.axis_index("ep") % 2
    place = jnp.stack([x, (x // 2 == core).astype(jnp.int32)]).astype(jnp.int32)

    first, second, swap = permutes(count_ep, count_tp)

    def send(weight, pairs):
        return lax.ppermute(weight, AXES, pairs)

    def spread(name, weight):
        moved = send(weight, first)
        other_own = send(weight, swap)
        other_moved = send(moved, swap)
        last = send(moved, second)
        other_last = send(last, swap)
        hold = in_vmem if name == "down" else in_hbm
        return (in_hbm(weight), in_hbm(other_own)), in_hbm(moved), in_hbm(other_moved), (hold(other_last), in_hbm(last))

    gate = spread("gate", gate_weight[0])
    up = spread("up", up_weight[0])
    down = spread("down", down_weight[0])

    buffer = dispatch_buffer(route_ids.T, in_gain[None, :], tokens, rows)
    received = lax.all_to_all(
        buffer.reshape(count_ep, rows, full_width), "ep", split_axis=0, concat_axis=0, tiled=True
    ).reshape(count_ep * rows, full_width)
    received = in_vmem(received)
    early = early_hidden(place, received, (*gate[0], gate[1], gate[2]), (*up[0], up[1], up[2]))
    middle = in_vmem(middle_hidden(place, received, gate[3], up[3]))
    outputs = late_outputs(
        place, early, middle, (*down[0], down[1], down[2], *down[3]), count_ep, count_tp
    )
    returned = lax.all_to_all(
        outputs.reshape(count_ep * count_tp, rows, part_width), AXES, split_axis=0, concat_axis=0, tiled=True
    ).reshape(count_ep * count_tp * rows, part_width)
    table = routing_table(route_ids, route_scores, rows, count_tp)
    combined, squares = combine(table, in_vmem(returned))
    parts = [squares] + [
        lax.ppermute(squares, "tp", [(i, (i + shift) % count_tp) for i in range(count_tp)])
        for shift in range(1, count_tp)
    ]
    return scale(combined, parts, out_gain[None, :], full_width)


def solution(mesh):
    in_specs = (
        P("ep", None),
        P(),
        P("ep", None),
        P("ep", None),
        P("ep", None, "tp"),
        P("ep", None, "tp"),
        P("ep", "tp", None),
        P("tp"),
    )
    out_specs = P("ep", "tp")
    return jax.shard_map(per_device, mesh=mesh, in_specs=in_specs, out_specs=out_specs, check_vma=False)
```

```python
import functools

import jax
import jax.numpy as jnp
from jax import lax
from jax.experimental import pallas as pl
from jax.experimental.pallas import tpu as pltpu
from jax.sharding import PartitionSpec as P


epsilon = 1e-06
AXES = ("ep", "tp")
MIB = 1024 * 1024


def place_of(ids, slot):
    ep = (ids // 2) * 2 + slot % 2
    tp = (ids % 2) * 2 + (slot % 4) // 2
    return ep, tp, slot // 4


def in_vmem(value):
    return pltpu.with_memory_space_constraint(value, pltpu.VMEM)


def in_hbm(value):
    return pltpu.with_memory_space_constraint(value, pltpu.HBM)


def permutes(count_ep, count_tp):
    def dev(ep, x):
        return ep * count_tp + x

    first, second, swap = [], [], []
    for ep in range(count_ep):
        core = ep % 2
        for x in range(count_tp):
            own = x // 2 == core
            swap.append((dev(ep, x), dev(ep ^ 1, x)))
            if own:
                first.append((dev(ep, x), dev(ep, x ^ 1)))
            else:
                first.append((dev(ep, x), dev(ep ^ 1, count_tp - 1 - x)))
                second.append((dev(ep, x), dev(ep, x ^ 1)))
    return first, second, swap


def dispatch_kernel(ids_ref, gain_ref, tokens_ref, out_ref, raw, pick, sems, *, rows, chunks):
    step = pl.program_id(0)
    count, _ = raw.shape
    part = count // chunks

    def load(i):
        return pltpu.make_async_copy(
            tokens_ref.at[pl.ds(i * part, part)], raw.at[pl.ds(i * part, part)], sems.at[i]
        )

    @pl.when(step == 0)
    def _():
        for i in range(chunks):
            load(i).start()
        experts = 32
        first = ids_ref[0:1, :]
        second = ids_ref[1:2, :]
        number = lax.broadcasted_iota(jnp.int32, (experts, count), 0)
        named_first = number == first
        named_second = number == second
        named = jnp.where(named_first | named_second, 1.0, 0.0).astype(jnp.bfloat16)
        before = lax.broadcasted_iota(jnp.int32, (count, count), 0) < lax.broadcasted_iota(
            jnp.int32, (count, count), 1
        )
        ranks = jnp.dot(
            named, jnp.where(before, 1.0, 0.0).astype(jnp.bfloat16), preferred_element_type=jnp.float32
        )
        slot_first = jnp.sum(jnp.where(named_first, ranks, 0.0), axis=0, keepdims=True).astype(jnp.int32)
        slot_second = jnp.sum(jnp.where(named_second, ranks, 0.0), axis=0, keepdims=True).astype(jnp.int32)
        mine = lax.axis_index("tp")

        def row_of(ids, slot):
            ep, tp, row = place_of(ids, slot)
            return jnp.where(tp == mine, ep * rows + row, -1)

        row_first = row_of(first, slot_first)
        row_second = row_of(second, slot_second)
        index = lax.broadcasted_iota(jnp.int32, (count, count), 0)
        pick[...] = jnp.where((index == row_first) | (index == row_second), 1.0, 0.0).astype(jnp.bfloat16)
        for i in range(chunks):
            load(i).wait()

    block = out_ref.shape[0]
    value = jnp.dot(pick[pl.ds(step * block, block), :], raw[...], preferred_element_type=jnp.float32)
    mean = jnp.mean(value * value, axis=1, keepdims=True)
    out_ref[...] = (value * lax.rsqrt(mean + epsilon) * gain_ref[...]).astype(jnp.bfloat16)


def dispatch_buffer(ids_rows, gain, tokens, rows):
    count, width = tokens.shape
    steps, chunks = 2, 2
    return pl.pallas_call(
        functools.partial(dispatch_kernel, rows=rows, chunks=chunks),
        grid=(steps,),
        in_specs=[
            pl.BlockSpec((2, count), lambda i: (0, 0)),
            pl.BlockSpec((1, width), lambda i: (0, 0)),
            pl.BlockSpec(memory_space=pltpu.HBM),
        ],
        out_specs=pl.BlockSpec((count // steps, width), lambda i: (i, 0)),
        scratch_shapes=[
            pltpu.VMEM((count, width), jnp.bfloat16),
            pltpu.VMEM((count, count), jnp.bfloat16),
            pltpu.SemaphoreType.DMA((chunks,)),
        ],
        out_shape=pltpu.HBM((count, width), jnp.bfloat16),
        compiler_params=pltpu.CompilerParams(dimension_semantics=("arbitrary",), vmem_limit_bytes=58 * MIB),
        name="dispatch_buffer",
    )(ids_rows, gain, tokens)


def start_one(flag, a, b, dst, sem):
    @pl.when(flag == 1)
    def _():
        pltpu.make_async_copy(a, dst, sem).start()

    @pl.when(flag != 1)
    def _():
        pltpu.make_async_copy(b, dst, sem).start()


def activation(acts, part):
    gate_acts = acts[:, :part]
    return (gate_acts / (1.0 + jnp.exp(-gate_acts)) * acts[:, part:]).astype(jnp.bfloat16)


def halves_of(width):
    return ((0, width // 2), (width // 2, width // 2))


def split_block(rows_ref, weights, waits):
    acts = None
    for (lo, size), wait in zip(halves_of(rows_ref.shape[1]), waits):
        wait()
        term = jnp.dot(
            rows_ref[:, lo : lo + size], weights[lo : lo + size, :], preferred_element_type=jnp.float32
        )
        acts = term if acts is None else acts + term
    return acts


def early_kernel(place_ref, rows_ref, ga, gb, g1, g2, ua, ub, u1, u2, out_ref, weights, sems):
    flag = place_ref[1]
    width, part = g1.shape

    def plain(at, lo, size, gate, up):
        for n, source in enumerate((gate, up)):
            yield (
                source.at[pl.ds(lo, size)],
                weights.at[at, pl.ds(lo, size), pl.ds(n * part, part)],
            )

    def wait_for(at, lo, size, sem):
        for n, (source, target) in enumerate(plain(at, lo, size, g1, u1)):
            pltpu.make_async_copy(source, target, sems.at[sem + n]).wait()

    for half, (lo, size) in enumerate(halves_of(width)):
        for n, (source, target) in enumerate(plain(0, lo, size, g1, u1)):
            pltpu.make_async_copy(source, target, sems.at[2 * half + n]).start()
    for n, (source, target) in enumerate(plain(1, 0, width, g2, u2)):
        pltpu.make_async_copy(source, target, sems.at[4 + n]).start()
    start_one(flag, ga, gb, weights.at[2, :, pl.ds(0, part)], sems.at[6])
    start_one(flag, ua, ub, weights.at[2, :, pl.ds(part, part)], sems.at[7])
    waits = [
        functools.partial(wait_for, 0, lo, size, 2 * half) for half, (lo, size) in enumerate(halves_of(width))
    ]
    out_ref[:, part : 2 * part] = activation(split_block(rows_ref, weights.at[0], waits), part)
    for at, out in ((1, 2), (2, 0)):
        wait_for(at, 0, width, 2 + 2 * at)
        acts = jnp.dot(rows_ref[...], weights[at], preferred_element_type=jnp.float32)
        out_ref[:, out * part : (out + 1) * part] = activation(acts, part)


def middle_kernel(place_ref, rows_ref, ga, gb, ua, ub, out_ref, weights, sems):
    flag = place_ref[1]
    width, part = ga.shape

    def target(lo, size, n):
        return weights.at[pl.ds(lo, size), pl.ds(n * part, part)]

    def wait_for(half, lo, size):
        for n in range(2):
            pltpu.make_async_copy(ga.at[pl.ds(lo, size)], target(lo, size, n), sems.at[2 * half + n]).wait()

    waits = []
    for half, (lo, size) in enumerate(halves_of(width)):
        for n, (a, b) in enumerate(((ga, gb), (ua, ub))):
            start_one(flag, a.at[pl.ds(lo, size)], b.at[pl.ds(lo, size)], target(lo, size, n), sems.at[2 * half + n])
        waits.append(functools.partial(wait_for, half, lo, size))
    out_ref[...] = activation(split_block(rows_ref, weights, waits), part)


HBM = pl.BlockSpec(memory_space=pltpu.HBM)
ANY = pl.BlockSpec(memory_space=pl.ANY)
SMEM = pl.BlockSpec(memory_space=pltpu.SMEM)
VMEM = pl.BlockSpec(memory_space=pltpu.VMEM)


def early_hidden(place, rows, gates, ups):
    count, width = rows.shape
    part = gates[0].shape[1]
    return pl.pallas_call(
        early_kernel,
        in_specs=[SMEM, VMEM] + [ANY] * 8,
        out_specs=VMEM,
        scratch_shapes=[pltpu.VMEM((3, width, 2 * part), jnp.bfloat16), pltpu.SemaphoreType.DMA((8,))],
        out_shape=pltpu.VMEM((count, 3 * part), jnp.bfloat16),
        compiler_params=pltpu.CompilerParams(vmem_limit_bytes=50 * MIB),
        name="early_hidden",
    )(place, rows, *gates, *ups)


def middle_hidden(place, rows, gates, ups):
    count, width = rows.shape
    part = gates[0].shape[1]
    return pl.pallas_call(
        middle_kernel,
        in_specs=[SMEM, VMEM] + [ANY] * 4,
        out_specs=VMEM,
        scratch_shapes=[pltpu.VMEM((width, 2 * part), jnp.bfloat16), pltpu.SemaphoreType.DMA((4,))],
        out_shape=jax.ShapeDtypeStruct((count, part), jnp.bfloat16),
        compiler_params=pltpu.CompilerParams(vmem_limit_bytes=50 * MIB),
        name="middle_hidden",
    )(place, rows, *gates, *ups)


def late_kernel(place_ref, early_ref, middle_ref, d0a, d0b, d1, d2, d3a, d3b, out_ref, down, hidden, out, sems, out_sems, *, cuts):
    flag = place_ref[1]
    senders, pieces, slots, piece = out_ref.shape
    part = d1.shape[0]
    size = piece // cuts
    steps = pieces * cuts

    def target(i, f):
        return down.at[pl.ds(i * part, part), pl.ds(f * size, size)]

    def source(ref, f):
        return ref.at[:, pl.ds(f * size, size)]

    for f in range(steps):
        pltpu.make_async_copy(source(d1, f), target(1, f), sems.at[4 * f + 1]).start()
        pltpu.make_async_copy(source(d2, f), target(2, f), sems.at[4 * f + 2]).start()
        start_one(flag, source(d0a, f), source(d0b, f), target(0, f), sems.at[4 * f])
        start_one(flag, source(d3a, f), source(d3b, f), target(3, f), sems.at[4 * f + 3])
    hidden[:, 0 : 3 * part] = early_ref[...]
    hidden[:, 3 * part : 4 * part] = middle_ref[...]

    def store(f):
        return pltpu.make_async_copy(
            out.at[f], out_ref.at[:, f // cuts, :, pl.ds(f % cuts * size, size)], out_sems.at[f]
        )

    for f in range(steps):
        for i in range(4):
            pltpu.make_async_copy(source(d1, f), target(i, f), sems.at[4 * f + i]).wait()
        value = jnp.dot(
            hidden[...], down[:, f * size : (f + 1) * size], preferred_element_type=jnp.float32
        )
        out[f] = value.reshape(senders, slots, size).astype(jnp.bfloat16)
        store(f).start()
    for f in range(steps):
        store(f).wait()


def late_outputs(place, early, middle, downs, senders, pieces):
    count = early.shape[0]
    part, width = downs[0].shape
    slots = count // senders
    piece = width // pieces
    shape = (senders, pieces, slots, piece)
    cuts = 1
    return pl.pallas_call(
        functools.partial(late_kernel, cuts=cuts),
        in_specs=[SMEM, VMEM, VMEM] + [ANY] * 6,
        out_specs=HBM,
        scratch_shapes=[
            pltpu.VMEM((4 * part, width), jnp.bfloat16),
            pltpu.VMEM((count, 4 * part), jnp.bfloat16),
            pltpu.VMEM((pieces * cuts, senders, slots, piece // cuts), jnp.bfloat16),
            pltpu.SemaphoreType.DMA((4 * pieces * cuts,)),
            pltpu.SemaphoreType.DMA((pieces * cuts,)),
        ],
        out_shape=pltpu.HBM(shape, jnp.bfloat16),
        compiler_params=pltpu.CompilerParams(vmem_limit_bytes=50 * MIB),
        name="late_outputs",
    )(place, early, middle, *downs)


def table_kernel(ids_ref, scores_ref, out_ref, *, rows, count_tp):
    count = ids_ref.shape[0]
    experts = 32
    first = ids_ref[:, 0:1]
    second = ids_ref[:, 1:2]
    number = lax.broadcasted_iota(jnp.int32, (count, experts), 1)
    named_first = number == first
    named_second = number == second
    named = jnp.where(named_first | named_second, 1.0, 0.0).astype(jnp.bfloat16)
    before = lax.broadcasted_iota(jnp.int32, (count, count), 1) < lax.broadcasted_iota(
        jnp.int32, (count, count), 0
    )
    ranks = jnp.dot(
        jnp.where(before, 1.0, 0.0).astype(jnp.bfloat16), named, preferred_element_type=jnp.float32
    )
    scores = scores_ref[...]
    out_ref[:, 2:4] = scores / jnp.sum(scores, axis=1, keepdims=True)
    for choice, (ids, chosen) in enumerate(((first, named_first), (second, named_second))):
        slot = jnp.sum(jnp.where(chosen, ranks, 0.0), axis=1, keepdims=True).astype(jnp.int32)
        ep, tp, row = place_of(ids, slot)
        out_ref[:, choice : choice + 1] = ((ep * count_tp + tp) * rows + row).astype(jnp.float32)


def routing_table(ids, scores, rows, count_tp):
    return pl.pallas_call(
        functools.partial(table_kernel, rows=rows, count_tp=count_tp),
        out_shape=jax.ShapeDtypeStruct((ids.shape[0], 4), jnp.float32),
        compiler_params=pltpu.CompilerParams(vmem_limit_bytes=16 * MIB),
        name="columns",
    )(ids, scores)


def combine_kernel(table_ref, returned_ref, out_ref, squares_ref):
    total = returned_ref.shape[0]
    count = table_ref.shape[0]
    index = lax.broadcasted_iota(jnp.int32, (count, total), 1)
    row = table_ref[:, 0:2].astype(jnp.int32)
    mix = table_ref[:, 2:4]
    hot = jnp.where(index == row[:, 0:1], mix[:, 0:1], jnp.where(index == row[:, 1:2], mix[:, 1:2], 0.0))
    value = jnp.dot(hot.astype(jnp.bfloat16), returned_ref[...], preferred_element_type=jnp.float32)
    out_ref[...] = value
    square = value * value
    lanes = 128
    folded = square[:, 0:lanes]
    for i in range(1, square.shape[1] // lanes):
        folded = folded + square[:, i * lanes : (i + 1) * lanes]
    squares_ref[...] = jnp.sum(folded.T, axis=0, keepdims=True)


def combine(table, returned):
    count = table.shape[0]
    piece = returned.shape[1]
    return pl.pallas_call(
        combine_kernel,
        in_specs=[VMEM, VMEM],
        out_specs=[VMEM, VMEM],
        out_shape=[
            pltpu.VMEM((count, piece), jnp.float32),
            jax.ShapeDtypeStruct((1, count), jnp.float32),
        ],
        compiler_params=pltpu.CompilerParams(vmem_limit_bytes=32 * MIB),
        name="combine",
    )(table, returned)


def scale_kernel(combined_ref, own_ref, a_ref, b_ref, c_ref, gain_ref, out_ref, *, width):
    total = own_ref[...] + a_ref[...] + b_ref[...] + c_ref[...]
    factor = lax.rsqrt(total / width + epsilon)
    count, piece = combined_ref.shape
    lanes = 128
    column = jnp.broadcast_to(factor, (lanes, count)).T
    for i in range(piece // lanes):
        at = slice(i * lanes, (i + 1) * lanes)
        out_ref[:, at] = (combined_ref[:, at] * column * gain_ref[:, at]).astype(jnp.bfloat16)


def scale(combined, squares, gain, width):
    count, piece = combined.shape
    return pl.pallas_call(
        functools.partial(scale_kernel, width=width),
        in_specs=[VMEM] * 6,
        out_specs=VMEM,
        out_shape=jax.ShapeDtypeStruct((count, piece), jnp.bfloat16),
        compiler_params=pltpu.CompilerParams(vmem_limit_bytes=16 * MIB),
        name="scale",
    )(combined, *squares, gain)


def per_device(
    tokens, in_gain, route_ids, route_scores, gate_weight, up_weight, down_weight, out_gain
):
    count_ep = lax.axis_size("ep")
    count_tp = lax.axis_size("tp")
    tok_count, full_width = tokens.shape
    part_width = full_width // count_tp
    capacity = 2 * tok_count * route_ids.shape[1] // count_ep
    rows = capacity // count_tp
    x = lax.axis_index("tp")
    core = lax.axis_index("ep") % 2
    place = jnp.stack([x, (x // 2 == core).astype(jnp.int32)]).astype(jnp.int32)

    first, second, swap = permutes(count_ep, count_tp)

    def send(weight, pairs):
        return lax.ppermute(weight, AXES, pairs)

    def spread(name, weight):
        moved = send(weight, first)
        other_own = send(weight, swap)
        other_moved = send(moved, swap)
        last = send(moved, second)
        other_last = send(last, swap)
        hold = in_vmem if name == "down" else in_hbm
        return (in_hbm(weight), in_hbm(other_own)), in_hbm(moved), in_hbm(other_moved), (hold(other_last), in_hbm(last))

    gate = spread("gate", gate_weight[0])
    up = spread("up", up_weight[0])
    down = spread("down", down_weight[0])

    buffer = dispatch_buffer(route_ids.T, in_gain[None, :], tokens, rows)
    received = lax.all_to_all(
        buffer.reshape(count_ep, rows, full_width), "ep", split_axis=0, concat_axis=0, tiled=True
    ).reshape(count_ep * rows, full_width)
    received = in_vmem(received)
    early = early_hidden(place, received, (*gate[0], gate[1], gate[2]), (*up[0], up[1], up[2]))
    middle = in_vmem(middle_hidden(place, received, gate[3], up[3]))
    outputs = late_outputs(
        place, early, middle, (*down[0], down[1], down[2], *down[3]), count_ep, count_tp
    )
    returned = lax.all_to_all(
        outputs.reshape(count_ep * count_tp, rows, part_width), AXES, split_axis=0, concat_axis=0, tiled=True
    ).reshape(count_ep * count_tp * rows, part_width)
    table = routing_table(route_ids, route_scores, rows, count_tp)
    combined, squares = combine(table, in_vmem(returned))
    parts = [squares] + [
        lax.ppermute(squares, "tp", [(i, (i + shift) % count_tp) for i in range(count_tp)])
        for shift in range(1, count_tp)
    ]
    return scale(combined, parts, out_gain[None, :], full_width)


def solution(mesh):
    in_specs = (
        P("ep", None),
        P(),
        P("ep", None),
        P("ep", None),
        P("ep", None, "tp"),
        P("ep", None, "tp"),
        P("ep", "tp", None),
        P("tp"),
    )
    out_specs = P("ep", "tp")
    return jax.shard_map(per_device, mesh=mesh, in_specs=in_specs, out_specs=out_specs, check_vma=False)
```

```python
import functools

import jax
import jax.numpy as jnp
from jax import lax
from jax.experimental import pallas as pl
from jax.experimental.pallas import tpu as pltpu
from jax.sharding import PartitionSpec as P


epsilon = 1e-06
AXES = ("ep", "tp")
MIB = 1024 * 1024


def place_of(ids, slot):
    ep = (ids // 2) * 2 + slot % 2
    tp = (ids % 2) * 2 + (slot % 4) // 2
    return ep, tp, slot // 4


def in_vmem(value):
    return pltpu.with_memory_space_constraint(value, pltpu.VMEM)


def in_hbm(value):
    return pltpu.with_memory_space_constraint(value, pltpu.HBM)


def permutes(count_ep, count_tp):
    def dev(ep, x):
        return ep * count_tp + x

    first, second, swap = [], [], []
    for ep in range(count_ep):
        core = ep % 2
        for x in range(count_tp):
            own = x // 2 == core
            swap.append((dev(ep, x), dev(ep ^ 1, x)))
            if own:
                first.append((dev(ep, x), dev(ep, x ^ 1)))
            else:
                first.append((dev(ep, x), dev(ep ^ 1, count_tp - 1 - x)))
                second.append((dev(ep, x), dev(ep, x ^ 1)))
    return first, second, swap


def dispatch_kernel(ids_ref, gain_ref, tokens_ref, out_ref, raw, pick, sems, *, rows, chunks):
    step = pl.program_id(0)
    count, _ = raw.shape
    part = count // chunks

    def load(i):
        return pltpu.make_async_copy(
            tokens_ref.at[pl.ds(i * part, part)], raw.at[pl.ds(i * part, part)], sems.at[i]
        )

    @pl.when(step == 0)
    def _():
        for i in range(chunks):
            load(i).start()
        experts = 32
        first = ids_ref[0:1, :]
        second = ids_ref[1:2, :]
        number = lax.broadcasted_iota(jnp.int32, (experts, count), 0)
        named_first = number == first
        named_second = number == second
        named = jnp.where(named_first | named_second, 1.0, 0.0).astype(jnp.bfloat16)
        before = lax.broadcasted_iota(jnp.int32, (count, count), 0) < lax.broadcasted_iota(
            jnp.int32, (count, count), 1
        )
        ranks = jnp.dot(
            named, jnp.where(before, 1.0, 0.0).astype(jnp.bfloat16), preferred_element_type=jnp.float32
        )
        slot_first = jnp.sum(jnp.where(named_first, ranks, 0.0), axis=0, keepdims=True).astype(jnp.int32)
        slot_second = jnp.sum(jnp.where(named_second, ranks, 0.0), axis=0, keepdims=True).astype(jnp.int32)
        mine = lax.axis_index("tp")

        def row_of(ids, slot):
            ep, tp, row = place_of(ids, slot)
            return jnp.where(tp == mine, ep * rows + row, -1)

        row_first = row_of(first, slot_first)
        row_second = row_of(second, slot_second)
        index = lax.broadcasted_iota(jnp.int32, (count, count), 0)
        pick[...] = jnp.where((index == row_first) | (index == row_second), 1.0, 0.0).astype(jnp.bfloat16)
        for i in range(chunks):
            load(i).wait()

    block = out_ref.shape[0]
    value = jnp.dot(pick[pl.ds(step * block, block), :], raw[...], preferred_element_type=jnp.float32)
    mean = jnp.mean(value * value, axis=1, keepdims=True)
    out_ref[...] = (value * lax.rsqrt(mean + epsilon) * gain_ref[...]).astype(jnp.bfloat16)


def dispatch_buffer(ids_rows, gain, tokens, rows):
    count, width = tokens.shape
    steps, chunks = 2, 2
    return pl.pallas_call(
        functools.partial(dispatch_kernel, rows=rows, chunks=chunks),
        grid=(steps,),
        in_specs=[
            pl.BlockSpec((2, count), lambda i: (0, 0)),
            pl.BlockSpec((1, width), lambda i: (0, 0)),
            pl.BlockSpec(memory_space=pltpu.HBM),
        ],
        out_specs=pl.BlockSpec((count // steps, width), lambda i: (i, 0)),
        scratch_shapes=[
            pltpu.VMEM((count, width), jnp.bfloat16),
            pltpu.VMEM((count, count), jnp.bfloat16),
            pltpu.SemaphoreType.DMA((chunks,)),
        ],
        out_shape=pltpu.HBM((count, width), jnp.bfloat16),
        compiler_params=pltpu.CompilerParams(dimension_semantics=("arbitrary",), vmem_limit_bytes=58 * MIB),
        name="dispatch_buffer",
    )(ids_rows, gain, tokens)


def start_one(flag, a, b, dst, sem):
    @pl.when(flag == 1)
    def _():
        pltpu.make_async_copy(a, dst, sem).start()

    @pl.when(flag != 1)
    def _():
        pltpu.make_async_copy(b, dst, sem).start()


def activation(acts, part):
    gate_acts = acts[:, :part]
    return (gate_acts / (1.0 + jnp.exp(-gate_acts)) * acts[:, part:]).astype(jnp.bfloat16)


def halves_of(width):
    return ((0, width // 2), (width // 2, width // 2))


def split_block(rows_ref, weights, waits):
    acts = None
    for (lo, size), wait in zip(halves_of(rows_ref.shape[1]), waits):
        wait()
        term = jnp.dot(
            rows_ref[:, lo : lo + size], weights[lo : lo + size, :], preferred_element_type=jnp.float32
        )
        acts = term if acts is None else acts + term
    return acts


def early_kernel(place_ref, rows_ref, ga, gb, g1, g2, ua, ub, u1, u2, out_ref, weights, sems):
    flag = place_ref[1]
    width, part = g1.shape

    def plain(at, lo, size, gate, up):
        for n, source in enumerate((gate, up)):
            yield (
                source.at[pl.ds(lo, size)],
                weights.at[at, pl.ds(lo, size), pl.ds(n * part, part)],
            )

    def wait_for(at, lo, size, sem):
        for n, (source, target) in enumerate(plain(at, lo, size, g1, u1)):
            pltpu.make_async_copy(source, target, sems.at[sem + n]).wait()

    for half, (lo, size) in enumerate(halves_of(width)):
        for n, (source, target) in enumerate(plain(0, lo, size, g1, u1)):
            pltpu.make_async_copy(source, target, sems.at[2 * half + n]).start()
    for n, (source, target) in enumerate(plain(1, 0, width, g2, u2)):
        pltpu.make_async_copy(source, target, sems.at[4 + n]).start()
    start_one(flag, ga, gb, weights.at[2, :, pl.ds(0, part)], sems.at[6])
    start_one(flag, ua, ub, weights.at[2, :, pl.ds(part, part)], sems.at[7])
    waits = [
        functools.partial(wait_for, 0, lo, size, 2 * half) for half, (lo, size) in enumerate(halves_of(width))
    ]
    out_ref[:, part : 2 * part] = activation(split_block(rows_ref, weights.at[0], waits), part)
    for at, out in ((1, 2), (2, 0)):
        wait_for(at, 0, width, 2 + 2 * at)
        acts = jnp.dot(rows_ref[...], weights[at], preferred_element_type=jnp.float32)
        out_ref[:, out * part : (out + 1) * part] = activation(acts, part)


def middle_kernel(place_ref, rows_ref, ga, gb, ua, ub, out_ref, weights, sems):
    flag = place_ref[1]
    width, part = ga.shape

    def target(lo, size, n):
        return weights.at[pl.ds(lo, size), pl.ds(n * part, part)]

    def wait_for(half, lo, size):
        for n in range(2):
            pltpu.make_async_copy(ga.at[pl.ds(lo, size)], target(lo, size, n), sems.at[2 * half + n]).wait()

    waits = []
    for half, (lo, size) in enumerate(halves_of(width)):
        for n, (a, b) in enumerate(((ga, gb), (ua, ub))):
            start_one(flag, a.at[pl.ds(lo, size)], b.at[pl.ds(lo, size)], target(lo, size, n), sems.at[2 * half + n])
        waits.append(functools.partial(wait_for, half, lo, size))
    out_ref[...] = activation(split_block(rows_ref, weights, waits), part)


HBM = pl.BlockSpec(memory_space=pltpu.HBM)
ANY = pl.BlockSpec(memory_space=pl.ANY)
SMEM = pl.BlockSpec(memory_space=pltpu.SMEM)
VMEM = pl.BlockSpec(memory_space=pltpu.VMEM)


def early_hidden(place, rows, gates, ups):
    count, width = rows.shape
    part = gates[0].shape[1]
    return pl.pallas_call(
        early_kernel,
        in_specs=[SMEM, VMEM] + [ANY] * 8,
        out_specs=VMEM,
        scratch_shapes=[pltpu.VMEM((3, width, 2 * part), jnp.bfloat16), pltpu.SemaphoreType.DMA((8,))],
        out_shape=pltpu.VMEM((count, 3 * part), jnp.bfloat16),
        compiler_params=pltpu.CompilerParams(vmem_limit_bytes=50 * MIB),
        name="early_hidden",
    )(place, rows, *gates, *ups)


def middle_hidden(place, rows, gates, ups):
    count, width = rows.shape
    part = gates[0].shape[1]
    return pl.pallas_call(
        middle_kernel,
        in_specs=[SMEM, VMEM] + [ANY] * 4,
        out_specs=VMEM,
        scratch_shapes=[pltpu.VMEM((width, 2 * part), jnp.bfloat16), pltpu.SemaphoreType.DMA((4,))],
        out_shape=jax.ShapeDtypeStruct((count, part), jnp.bfloat16),
        compiler_params=pltpu.CompilerParams(vmem_limit_bytes=50 * MIB),
        name="middle_hidden",
    )(place, rows, *gates, *ups)


def late_kernel(place_ref, early_ref, middle_ref, d0a, d0b, d1, d2, d3a, d3b, out_ref, down, hidden, out, sems, out_sems, *, cuts):
    flag = place_ref[1]
    senders, pieces, slots, piece = out_ref.shape
    part = d1.shape[0]
    size = piece // cuts
    steps = pieces * cuts

    def target(i, f):
        return down.at[pl.ds(i * part, part), pl.ds(f * size, size)]

    def source(ref, f):
        return ref.at[:, pl.ds(f * size, size)]

    for f in range(steps):
        pltpu.make_async_copy(source(d1, f), target(1, f), sems.at[4 * f + 1]).start()
        pltpu.make_async_copy(source(d2, f), target(2, f), sems.at[4 * f + 2]).start()
        start_one(flag, source(d0a, f), source(d0b, f), target(0, f), sems.at[4 * f])
        start_one(flag, source(d3a, f), source(d3b, f), target(3, f), sems.at[4 * f + 3])
    hidden[:, 0 : 3 * part] = early_ref[...]
    hidden[:, 3 * part : 4 * part] = middle_ref[...]

    def store(f):
        return pltpu.make_async_copy(
            out.at[f], out_ref.at[:, f // cuts, :, pl.ds(f % cuts * size, size)], out_sems.at[f]
        )

    for f in range(steps):
        for i in range(4):
            pltpu.make_async_copy(source(d1, f), target(i, f), sems.at[4 * f + i]).wait()
        value = jnp.dot(
            hidden[...], down[:, f * size : (f + 1) * size], preferred_element_type=jnp.float32
        )
        out[f] = value.reshape(senders, slots, size).astype(jnp.bfloat16)
        store(f).start()
    for f in range(steps):
        store(f).wait()


def late_outputs(place, early, middle, downs, senders, pieces):
    count = early.shape[0]
    part, width = downs[0].shape
    slots = count // senders
    piece = width // pieces
    shape = (senders, pieces, slots, piece)
    cuts = 1
    return pl.pallas_call(
        functools.partial(late_kernel, cuts=cuts),
        in_specs=[SMEM, VMEM, VMEM] + [ANY] * 6,
        out_specs=HBM,
        scratch_shapes=[
            pltpu.VMEM((4 * part, width), jnp.bfloat16),
            pltpu.VMEM((count, 4 * part), jnp.bfloat16),
            pltpu.VMEM((pieces * cuts, senders, slots, piece // cuts), jnp.bfloat16),
            pltpu.SemaphoreType.DMA((4 * pieces * cuts,)),
            pltpu.SemaphoreType.DMA((pieces * cuts,)),
        ],
        out_shape=pltpu.HBM(shape, jnp.bfloat16),
        compiler_params=pltpu.CompilerParams(vmem_limit_bytes=50 * MIB),
        name="late_outputs",
    )(place, early, middle, *downs)


def table_kernel(ids_ref, scores_ref, out_ref, *, rows, count_tp):
    count = ids_ref.shape[0]
    experts = 32
    first = ids_ref[:, 0:1]
    second = ids_ref[:, 1:2]
    number = lax.broadcasted_iota(jnp.int32, (count, experts), 1)
    named_first = number == first
    named_second = number == second
    named = jnp.where(named_first | named_second, 1.0, 0.0).astype(jnp.bfloat16)
    before = lax.broadcasted_iota(jnp.int32, (count, count), 1) < lax.broadcasted_iota(
        jnp.int32, (count, count), 0
    )
    ranks = jnp.dot(
        jnp.where(before, 1.0, 0.0).astype(jnp.bfloat16), named, preferred_element_type=jnp.float32
    )
    scores = scores_ref[...]
    out_ref[:, 2:4] = scores / jnp.sum(scores, axis=1, keepdims=True)
    for choice, (ids, chosen) in enumerate(((first, named_first), (second, named_second))):
        slot = jnp.sum(jnp.where(chosen, ranks, 0.0), axis=1, keepdims=True).astype(jnp.int32)
        ep, tp, row = place_of(ids, slot)
        out_ref[:, choice : choice + 1] = ((ep * count_tp + tp) * rows + row).astype(jnp.float32)


def routing_table(ids, scores, rows, count_tp):
    return pl.pallas_call(
        functools.partial(table_kernel, rows=rows, count_tp=count_tp),
        out_shape=jax.ShapeDtypeStruct((ids.shape[0], 4), jnp.float32),
        compiler_params=pltpu.CompilerParams(vmem_limit_bytes=16 * MIB),
        name="columns",
    )(ids, scores)


def combine_kernel(table_ref, returned_ref, out_ref, squares_ref):
    total = returned_ref.shape[0]
    count = table_ref.shape[0]
    index = lax.broadcasted_iota(jnp.int32, (count, total), 1)
    row = table_ref[:, 0:2].astype(jnp.int32)
    mix = table_ref[:, 2:4]
    hot = jnp.where(index == row[:, 0:1], mix[:, 0:1], jnp.where(index == row[:, 1:2], mix[:, 1:2], 0.0))
    value = jnp.dot(hot.astype(jnp.bfloat16), returned_ref[...], preferred_element_type=jnp.float32)
    out_ref[...] = value
    square = value * value
    lanes = 128
    folded = square[:, 0:lanes]
    for i in range(1, square.shape[1] // lanes):
        folded = folded + square[:, i * lanes : (i + 1) * lanes]
    squares_ref[...] = jnp.sum(folded.T, axis=0, keepdims=True)


def combine(table, returned):
    count = table.shape[0]
    piece = returned.shape[1]
    return pl.pallas_call(
        combine_kernel,
        in_specs=[VMEM, VMEM],
        out_specs=[VMEM, VMEM],
        out_shape=[
            pltpu.VMEM((count, piece), jnp.float32),
            jax.ShapeDtypeStruct((1, count), jnp.float32),
        ],
        compiler_params=pltpu.CompilerParams(vmem_limit_bytes=32 * MIB),
        name="combine",
    )(table, returned)


def scale_kernel(combined_ref, pair_ref, other_ref, gain_ref, out_ref, *, width):
    total = pair_ref[...] + other_ref[...]
    factor = lax.rsqrt(total / width + epsilon)
    count, piece = combined_ref.shape
    lanes = 128
    column = jnp.broadcast_to(factor, (lanes, count)).T
    for i in range(piece // lanes):
        at = slice(i * lanes, (i + 1) * lanes)
        out_ref[:, at] = (combined_ref[:, at] * column * gain_ref[:, at]).astype(jnp.bfloat16)


def scale(combined, pair, other, gain, width):
    count, piece = combined.shape
    return pl.pallas_call(
        functools.partial(scale_kernel, width=width),
        in_specs=[VMEM] * 4,
        out_specs=VMEM,
        out_shape=jax.ShapeDtypeStruct((count, piece), jnp.bfloat16),
        compiler_params=pltpu.CompilerParams(vmem_limit_bytes=16 * MIB),
        name="scale",
    )(combined, pair, other, gain)


def per_device(
    tokens, in_gain, route_ids, route_scores, gate_weight, up_weight, down_weight, out_gain
):
    count_ep = lax.axis_size("ep")
    count_tp = lax.axis_size("tp")
    tok_count, full_width = tokens.shape
    part_width = full_width // count_tp
    capacity = 2 * tok_count * route_ids.shape[1] // count_ep
    rows = capacity // count_tp
    x = lax.axis_index("tp")
    core = lax.axis_index("ep") % 2
    place = jnp.stack([x, (x // 2 == core).astype(jnp.int32)]).astype(jnp.int32)

    first, second, swap = permutes(count_ep, count_tp)

    def send(weight, pairs):
        return lax.ppermute(weight, AXES, pairs)

    def spread(name, weight):
        moved = send(weight, first)
        other_own = send(weight, swap)
        other_moved = send(moved, swap)
        last = send(moved, second)
        other_last = send(last, swap)
        hold = in_vmem if name == "down" else in_hbm
        return (in_hbm(weight), in_hbm(other_own)), in_hbm(moved), in_hbm(other_moved), (hold(other_last), in_hbm(last))

    gate = spread("gate", gate_weight[0])
    up = spread("up", up_weight[0])
    down = spread("down", down_weight[0])

    buffer = dispatch_buffer(route_ids.T, in_gain[None, :], tokens, rows)
    received = lax.all_to_all(
        buffer.reshape(count_ep, rows, full_width), "ep", split_axis=0, concat_axis=0, tiled=True
    ).reshape(count_ep * rows, full_width)
    received = in_vmem(received)
    early = early_hidden(place, received, (*gate[0], gate[1], gate[2]), (*up[0], up[1], up[2]))
    middle = in_vmem(middle_hidden(place, received, gate[3], up[3]))
    outputs = late_outputs(
        place, early, middle, (*down[0], down[1], down[2], *down[3]), count_ep, count_tp
    )
    returned = lax.all_to_all(
        outputs.reshape(count_ep * count_tp, rows, part_width), AXES, split_axis=0, concat_axis=0, tiled=True
    ).reshape(count_ep * count_tp * rows, part_width)
    table = routing_table(route_ids, route_scores, rows, count_tp)
    combined, squares = combine(table, in_vmem(returned))
    pair = squares + lax.ppermute(squares, "tp", [(i, i ^ 1) for i in range(count_tp)])
    other = lax.ppermute(pair, "tp", [(i, count_tp - 1 - i) for i in range(count_tp)])
    return scale(combined, pair, other, out_gain[None, :], full_width)


def solution(mesh):
    in_specs = (
        P("ep", None),
        P(),
        P("ep", None),
        P("ep", None),
        P("ep", None, "tp"),
        P("ep", None, "tp"),
        P("ep", "tp", None),
        P("tp"),
    )
    out_specs = P("ep", "tp")
    return jax.shard_map(per_device, mesh=mesh, in_specs=in_specs, out_specs=out_specs, check_vma=False)
```

```python
import functools

import jax
import jax.numpy as jnp
from jax import lax
from jax.experimental import pallas as pl
from jax.experimental.pallas import tpu as pltpu
from jax.sharding import PartitionSpec as P


epsilon = 1e-06
AXES = ("ep", "tp")
MIB = 1024 * 1024


def place_of(ids, slot):
    ep = (ids // 2) * 2 + slot % 2
    tp = (ids % 2) * 2 + (slot % 4) // 2
    return ep, tp, slot // 4


def in_vmem(value):
    return pltpu.with_memory_space_constraint(value, pltpu.VMEM)


def in_hbm(value):
    return pltpu.with_memory_space_constraint(value, pltpu.HBM)


def permutes(count_ep, count_tp):
    def dev(ep, x):
        return ep * count_tp + x

    first, second, swap = [], [], []
    for ep in range(count_ep):
        core = ep % 2
        for x in range(count_tp):
            own = x // 2 == core
            swap.append((dev(ep, x), dev(ep ^ 1, x)))
            if own:
                first.append((dev(ep, x), dev(ep, x ^ 1)))
            else:
                first.append((dev(ep, x), dev(ep ^ 1, count_tp - 1 - x)))
                second.append((dev(ep, x), dev(ep, x ^ 1)))
    return first, second, swap


def dispatch_kernel(ids_ref, gain_ref, tokens_ref, out_ref, raw, pick, sems, *, rows, chunks):
    step = pl.program_id(0)
    count, _ = raw.shape
    part = count // chunks

    def load(i):
        return pltpu.make_async_copy(
            tokens_ref.at[pl.ds(i * part, part)], raw.at[pl.ds(i * part, part)], sems.at[i]
        )

    @pl.when(step == 0)
    def _():
        for i in range(chunks):
            load(i).start()
        experts = 32
        first = ids_ref[0:1, :]
        second = ids_ref[1:2, :]
        number = lax.broadcasted_iota(jnp.int32, (experts, count), 0)
        named_first = number == first
        named_second = number == second
        named = jnp.where(named_first | named_second, 1.0, 0.0).astype(jnp.bfloat16)
        before = lax.broadcasted_iota(jnp.int32, (count, count), 0) < lax.broadcasted_iota(
            jnp.int32, (count, count), 1
        )
        ranks = jnp.dot(
            named, jnp.where(before, 1.0, 0.0).astype(jnp.bfloat16), preferred_element_type=jnp.float32
        )
        slot_first = jnp.sum(jnp.where(named_first, ranks, 0.0), axis=0, keepdims=True).astype(jnp.int32)
        slot_second = jnp.sum(jnp.where(named_second, ranks, 0.0), axis=0, keepdims=True).astype(jnp.int32)
        mine = lax.axis_index("tp")

        def row_of(ids, slot):
            ep, tp, row = place_of(ids, slot)
            return jnp.where(tp == mine, ep * rows + row, -1)

        row_first = row_of(first, slot_first)
        row_second = row_of(second, slot_second)
        index = lax.broadcasted_iota(jnp.int32, (count, count), 0)
        pick[...] = jnp.where((index == row_first) | (index == row_second), 1.0, 0.0).astype(jnp.bfloat16)
        for i in range(chunks):
            load(i).wait()

    block = out_ref.shape[0]
    value = jnp.dot(pick[pl.ds(step * block, block), :], raw[...], preferred_element_type=jnp.float32)
    mean = jnp.mean(value * value, axis=1, keepdims=True)
    out_ref[...] = (value * lax.rsqrt(mean + epsilon) * gain_ref[...]).astype(jnp.bfloat16)


def dispatch_buffer(ids_rows, gain, tokens, rows):
    count, width = tokens.shape
    steps, chunks = 2, 2
    return pl.pallas_call(
        functools.partial(dispatch_kernel, rows=rows, chunks=chunks),
        grid=(steps,),
        in_specs=[
            pl.BlockSpec((2, count), lambda i: (0, 0)),
            pl.BlockSpec((1, width), lambda i: (0, 0)),
            pl.BlockSpec(memory_space=pltpu.HBM),
        ],
        out_specs=pl.BlockSpec((count // steps, width), lambda i: (i, 0)),
        scratch_shapes=[
            pltpu.VMEM((count, width), jnp.bfloat16),
            pltpu.VMEM((count, count), jnp.bfloat16),
            pltpu.SemaphoreType.DMA((chunks,)),
        ],
        out_shape=pltpu.HBM((count, width), jnp.bfloat16),
        compiler_params=pltpu.CompilerParams(dimension_semantics=("arbitrary",), vmem_limit_bytes=58 * MIB),
        name="dispatch_buffer",
    )(ids_rows, gain, tokens)


def start_one(flag, a, b, dst, sem):
    @pl.when(flag == 1)
    def _():
        pltpu.make_async_copy(a, dst, sem).start()

    @pl.when(flag != 1)
    def _():
        pltpu.make_async_copy(b, dst, sem).start()


def activation(acts, part):
    gate_acts = acts[:, :part]
    return (gate_acts / (1.0 + jnp.exp(-gate_acts)) * acts[:, part:]).astype(jnp.bfloat16)


def halves_of(width):
    return ((0, width // 2), (width // 2, width // 2))


def split_block(rows_ref, weights, waits):
    acts = None
    for (lo, size), wait in zip(halves_of(rows_ref.shape[1]), waits):
        wait()
        term = jnp.dot(
            rows_ref[:, lo : lo + size], weights[lo : lo + size, :], preferred_element_type=jnp.float32
        )
        acts = term if acts is None else acts + term
    return acts


def early_kernel(
    place_ref, rows_ref, ga, gb, g1, g2, ua, ub, u1, u2, d0a, d0b, d1, d2, out_ref, down_ref, weights, sems
):
    flag = place_ref[1]
    width, part = g1.shape

    def plain(at, lo, size, gate, up):
        for n, source in enumerate((gate, up)):
            yield (
                source.at[pl.ds(lo, size)],
                weights.at[at, pl.ds(lo, size), pl.ds(n * part, part)],
            )

    def wait_for(at, lo, size, sem):
        for n, (source, target) in enumerate(plain(at, lo, size, g1, u1)):
            pltpu.make_async_copy(source, target, sems.at[sem + n]).wait()

    for half, (lo, size) in enumerate(halves_of(width)):
        for n, (source, target) in enumerate(plain(0, lo, size, g1, u1)):
            pltpu.make_async_copy(source, target, sems.at[2 * half + n]).start()
    for n, (source, target) in enumerate(plain(1, 0, width, g2, u2)):
        pltpu.make_async_copy(source, target, sems.at[4 + n]).start()
    start_one(flag, ga, gb, weights.at[2, :, pl.ds(0, part)], sems.at[6])
    start_one(flag, ua, ub, weights.at[2, :, pl.ds(part, part)], sems.at[7])
    start_one(flag, d0a, d0b, down_ref.at[pl.ds(0, part)], sems.at[8])
    pltpu.make_async_copy(d1, down_ref.at[pl.ds(part, part)], sems.at[9]).start()
    pltpu.make_async_copy(d2, down_ref.at[pl.ds(2 * part, part)], sems.at[10]).start()
    waits = [
        functools.partial(wait_for, 0, lo, size, 2 * half) for half, (lo, size) in enumerate(halves_of(width))
    ]
    out_ref[:, part : 2 * part] = activation(split_block(rows_ref, weights.at[0], waits), part)
    for at, out in ((1, 2), (2, 0)):
        wait_for(at, 0, width, 2 + 2 * at)
        acts = jnp.dot(rows_ref[...], weights[at], preferred_element_type=jnp.float32)
        out_ref[:, out * part : (out + 1) * part] = activation(acts, part)
    for i in range(3):
        pltpu.make_async_copy(d1, down_ref.at[pl.ds(i * part, part)], sems.at[8 + i]).wait()


def middle_kernel(place_ref, rows_ref, ga, gb, ua, ub, out_ref, weights, sems):
    flag = place_ref[1]
    width, part = ga.shape

    def target(lo, size, n):
        return weights.at[pl.ds(lo, size), pl.ds(n * part, part)]

    def wait_for(half, lo, size):
        for n in range(2):
            pltpu.make_async_copy(ga.at[pl.ds(lo, size)], target(lo, size, n), sems.at[2 * half + n]).wait()

    waits = []
    for half, (lo, size) in enumerate(halves_of(width)):
        for n, (a, b) in enumerate(((ga, gb), (ua, ub))):
            start_one(flag, a.at[pl.ds(lo, size)], b.at[pl.ds(lo, size)], target(lo, size, n), sems.at[2 * half + n])
        waits.append(functools.partial(wait_for, half, lo, size))
    out_ref[...] = activation(split_block(rows_ref, weights, waits), part)


HBM = pl.BlockSpec(memory_space=pltpu.HBM)
ANY = pl.BlockSpec(memory_space=pl.ANY)
SMEM = pl.BlockSpec(memory_space=pltpu.SMEM)
VMEM = pl.BlockSpec(memory_space=pltpu.VMEM)


def early_hidden(place, rows, gates, ups, downs):
    count, width = rows.shape
    part = gates[0].shape[1]
    return pl.pallas_call(
        early_kernel,
        in_specs=[SMEM, VMEM] + [ANY] * 12,
        out_specs=[VMEM, VMEM],
        scratch_shapes=[pltpu.VMEM((3, width, 2 * part), jnp.bfloat16), pltpu.SemaphoreType.DMA((11,))],
        out_shape=[pltpu.VMEM((count, 3 * part), jnp.bfloat16), pltpu.VMEM((3 * part, width), jnp.bfloat16)],
        compiler_params=pltpu.CompilerParams(vmem_limit_bytes=32 * MIB),
        name="early_hidden",
    )(place, rows, *gates, *ups, *downs)


def middle_hidden(place, rows, gates, ups):
    count, width = rows.shape
    part = gates[0].shape[1]
    return pl.pallas_call(
        middle_kernel,
        in_specs=[SMEM, VMEM] + [ANY] * 4,
        out_specs=VMEM,
        scratch_shapes=[pltpu.VMEM((width, 2 * part), jnp.bfloat16), pltpu.SemaphoreType.DMA((4,))],
        out_shape=jax.ShapeDtypeStruct((count, part), jnp.bfloat16),
        compiler_params=pltpu.CompilerParams(vmem_limit_bytes=32 * MIB),
        name="middle_hidden",
    )(place, rows, *gates, *ups)


def late_kernel(place_ref, early_ref, middle_ref, down_ref, d3a, d3b, out_ref, last, out, sems, out_sems):
    flag = place_ref[1]
    pieces, senders, slots, piece = out.shape

    def columns(ref, f):
        return ref.at[:, pl.ds(f * piece, piece)]

    def store(f):
        return pltpu.make_async_copy(out.at[f], out_ref.at[:, f], out_sems.at[f])

    for f in range(pieces):
        start_one(flag, columns(d3a, f), columns(d3b, f), columns(last, f), sems.at[f])
    for f in range(pieces):
        at = slice(f * piece, (f + 1) * piece)
        value = jnp.dot(early_ref[...], down_ref[:, at], preferred_element_type=jnp.float32)
        pltpu.make_async_copy(columns(d3a, f), columns(last, f), sems.at[f]).wait()
        value = value + jnp.dot(middle_ref[...], last[:, at], preferred_element_type=jnp.float32)
        out[f] = value.reshape(senders, slots, piece).astype(jnp.bfloat16)
        store(f).start()
    for f in range(pieces):
        store(f).wait()


def late_outputs(place, early, middle, down, lasts, senders, pieces):
    count = early.shape[0]
    part, width = lasts[0].shape
    slots = count // senders
    piece = width // pieces
    shape = (senders, pieces, slots, piece)
    return pl.pallas_call(
        late_kernel,
        in_specs=[SMEM, VMEM, VMEM, VMEM, ANY, ANY],
        out_specs=HBM,
        scratch_shapes=[
            pltpu.VMEM((part, width), jnp.bfloat16),
            pltpu.VMEM((pieces, senders, slots, piece), jnp.bfloat16),
            pltpu.SemaphoreType.DMA((pieces,)),
            pltpu.SemaphoreType.DMA((pieces,)),
        ],
        out_shape=pltpu.HBM(shape, jnp.bfloat16),
        compiler_params=pltpu.CompilerParams(vmem_limit_bytes=32 * MIB),
        name="late_outputs",
    )(place, early, middle, down, *lasts)


def table_kernel(ids_ref, scores_ref, out_ref, *, rows, count_tp):
    count = ids_ref.shape[0]
    experts = 32
    first = ids_ref[:, 0:1]
    second = ids_ref[:, 1:2]
    number = lax.broadcasted_iota(jnp.int32, (count, experts), 1)
    named_first = number == first
    named_second = number == second
    named = jnp.where(named_first | named_second, 1.0, 0.0).astype(jnp.bfloat16)
    before = lax.broadcasted_iota(jnp.int32, (count, count), 1) < lax.broadcasted_iota(
        jnp.int32, (count, count), 0
    )
    ranks = jnp.dot(
        jnp.where(before, 1.0, 0.0).astype(jnp.bfloat16), named, preferred_element_type=jnp.float32
    )
    scores = scores_ref[...]
    out_ref[:, 2:4] = scores / jnp.sum(scores, axis=1, keepdims=True)
    for choice, (ids, chosen) in enumerate(((first, named_first), (second, named_second))):
        slot = jnp.sum(jnp.where(chosen, ranks, 0.0), axis=1, keepdims=True).astype(jnp.int32)
        ep, tp, row = place_of(ids, slot)
        out_ref[:, choice : choice + 1] = ((ep * count_tp + tp) * rows + row).astype(jnp.float32)


def routing_table(ids, scores, rows, count_tp):
    return pl.pallas_call(
        functools.partial(table_kernel, rows=rows, count_tp=count_tp),
        out_shape=jax.ShapeDtypeStruct((ids.shape[0], 4), jnp.float32),
        compiler_params=pltpu.CompilerParams(vmem_limit_bytes=16 * MIB),
        name="columns",
    )(ids, scores)


def combine_kernel(table_ref, returned_ref, out_ref, squares_ref):
    total = returned_ref.shape[0]
    count = table_ref.shape[0]
    index = lax.broadcasted_iota(jnp.int32, (count, total), 1)
    row = table_ref[:, 0:2].astype(jnp.int32)
    mix = table_ref[:, 2:4]
    hot = jnp.where(index == row[:, 0:1], mix[:, 0:1], jnp.where(index == row[:, 1:2], mix[:, 1:2], 0.0))
    value = jnp.dot(hot.astype(jnp.bfloat16), returned_ref[...], preferred_element_type=jnp.float32)
    out_ref[...] = value
    square = value * value
    lanes = 128
    folded = square[:, 0:lanes]
    for i in range(1, square.shape[1] // lanes):
        folded = folded + square[:, i * lanes : (i + 1) * lanes]
    squares_ref[...] = jnp.sum(folded.T, axis=0, keepdims=True)


def combine(table, returned):
    count = table.shape[0]
    piece = returned.shape[1]
    return pl.pallas_call(
        combine_kernel,
        in_specs=[VMEM, VMEM],
        out_specs=[VMEM, VMEM],
        out_shape=[
            pltpu.VMEM((count, piece), jnp.float32),
            jax.ShapeDtypeStruct((1, count), jnp.float32),
        ],
        compiler_params=pltpu.CompilerParams(vmem_limit_bytes=32 * MIB),
        name="combine",
    )(table, returned)


def scale_kernel(combined_ref, own_ref, a_ref, b_ref, c_ref, gain_ref, out_ref, *, width):
    total = own_ref[...] + a_ref[...] + b_ref[...] + c_ref[...]
    factor = lax.rsqrt(total / width + epsilon)
    count, piece = combined_ref.shape
    lanes = 128
    column = jnp.broadcast_to(factor, (lanes, count)).T
    for i in range(piece // lanes):
        at = slice(i * lanes, (i + 1) * lanes)
        out_ref[:, at] = (combined_ref[:, at] * column * gain_ref[:, at]).astype(jnp.bfloat16)


def scale(combined, squares, gain, width):
    count, piece = combined.shape
    return pl.pallas_call(
        functools.partial(scale_kernel, width=width),
        in_specs=[VMEM] * 6,
        out_specs=VMEM,
        out_shape=jax.ShapeDtypeStruct((count, piece), jnp.bfloat16),
        compiler_params=pltpu.CompilerParams(vmem_limit_bytes=16 * MIB),
        name="scale",
    )(combined, *squares, gain)


def per_device(
    tokens, in_gain, route_ids, route_scores, gate_weight, up_weight, down_weight, out_gain
):
    count_ep = lax.axis_size("ep")
    count_tp = lax.axis_size("tp")
    tok_count, full_width = tokens.shape
    part_width = full_width // count_tp
    capacity = 2 * tok_count * route_ids.shape[1] // count_ep
    rows = capacity // count_tp
    x = lax.axis_index("tp")
    core = lax.axis_index("ep") % 2
    place = jnp.stack([x, (x // 2 == core).astype(jnp.int32)]).astype(jnp.int32)

    first, second, swap = permutes(count_ep, count_tp)

    def send(weight, pairs):
        return lax.ppermute(weight, AXES, pairs)

    def spread(name, weight):
        moved = send(weight, first)
        other_own = send(weight, swap)
        other_moved = send(moved, swap)
        last = send(moved, second)
        other_last = send(last, swap)
        hold = in_vmem if name == "down" else in_hbm
        return (in_hbm(weight), in_hbm(other_own)), in_hbm(moved), in_hbm(other_moved), (hold(other_last), in_hbm(last))

    gate = spread("gate", gate_weight[0])
    up = spread("up", up_weight[0])
    down = spread("down", down_weight[0])

    buffer = dispatch_buffer(route_ids.T, in_gain[None, :], tokens, rows)
    received = lax.all_to_all(
        buffer.reshape(count_ep, rows, full_width), "ep", split_axis=0, concat_axis=0, tiled=True
    ).reshape(count_ep * rows, full_width)
    received = in_vmem(received)
    early, loaded = early_hidden(
        place, received, (*gate[0], gate[1], gate[2]), (*up[0], up[1], up[2]), (*down[0], down[1], down[2])
    )
    middle = in_vmem(middle_hidden(place, received, gate[3], up[3]))
    outputs = late_outputs(
        place, early, middle, loaded, down[3], count_ep, count_tp
    )
    returned = lax.all_to_all(
        outputs.reshape(count_ep * count_tp, rows, part_width), AXES, split_axis=0, concat_axis=0, tiled=True
    ).reshape(count_ep * count_tp * rows, part_width)
    table = routing_table(route_ids, route_scores, rows, count_tp)
    combined, squares = combine(table, in_vmem(returned))
    parts = [squares] + [
        lax.ppermute(squares, "tp", [(i, (i + shift) % count_tp) for i in range(count_tp)])
        for shift in (1, count_tp - 1, 2)
    ]
    return scale(combined, parts, out_gain[None, :], full_width)


def solution(mesh):
    in_specs = (
        P("ep", None),
        P(),
        P("ep", None),
        P("ep", None),
        P("ep", None, "tp"),
        P("ep", None, "tp"),
        P("ep", "tp", None),
        P("tp"),
    )
    out_specs = P("ep", "tp")
    return jax.shard_map(per_device, mesh=mesh, in_specs=in_specs, out_specs=out_specs, check_vma=False)
```

```python
import functools

import jax
import jax.numpy as jnp
from jax import lax
from jax.experimental import pallas as pl
from jax.experimental.pallas import tpu as pltpu
from jax.sharding import PartitionSpec as P


epsilon = 1e-06
AXES = ("ep", "tp")
MIB = 1024 * 1024


def place_of(ids, slot):
    ep = (ids // 2) * 2 + slot % 2
    tp = (ids % 2) * 2 + (slot % 4) // 2
    return ep, tp, slot // 4


def in_vmem(value):
    return pltpu.with_memory_space_constraint(value, pltpu.VMEM)


def in_hbm(value):
    return pltpu.with_memory_space_constraint(value, pltpu.HBM)


def permutes(count_ep, count_tp):
    def dev(ep, x):
        return ep * count_tp + x

    first, second, swap = [], [], []
    for ep in range(count_ep):
        core = ep % 2
        for x in range(count_tp):
            own = x // 2 == core
            swap.append((dev(ep, x), dev(ep ^ 1, x)))
            if own:
                first.append((dev(ep, x), dev(ep, x ^ 1)))
            else:
                first.append((dev(ep, x), dev(ep ^ 1, count_tp - 1 - x)))
                second.append((dev(ep, x), dev(ep, x ^ 1)))
    return first, second, swap


def dispatch_kernel(ids_ref, gain_ref, tokens_ref, out_ref, raw, pick, sems, *, rows, chunks):
    step = pl.program_id(0)
    count, _ = raw.shape
    part = count // chunks

    def load(i):
        return pltpu.make_async_copy(
            tokens_ref.at[pl.ds(i * part, part)], raw.at[pl.ds(i * part, part)], sems.at[i]
        )

    @pl.when(step == 0)
    def _():
        for i in range(chunks):
            load(i).start()
        experts = 32
        first = ids_ref[0:1, :]
        second = ids_ref[1:2, :]
        number = lax.broadcasted_iota(jnp.int32, (experts, count), 0)
        named_first = number == first
        named_second = number == second
        named = jnp.where(named_first | named_second, 1.0, 0.0).astype(jnp.bfloat16)
        before = lax.broadcasted_iota(jnp.int32, (count, count), 0) < lax.broadcasted_iota(
            jnp.int32, (count, count), 1
        )
        ranks = jnp.dot(
            named, jnp.where(before, 1.0, 0.0).astype(jnp.bfloat16), preferred_element_type=jnp.float32
        )
        slot_first = jnp.sum(jnp.where(named_first, ranks, 0.0), axis=0, keepdims=True).astype(jnp.int32)
        slot_second = jnp.sum(jnp.where(named_second, ranks, 0.0), axis=0, keepdims=True).astype(jnp.int32)
        mine = lax.axis_index("tp")

        def row_of(ids, slot):
            ep, tp, row = place_of(ids, slot)
            return jnp.where(tp == mine, ep * rows + row, -1)

        row_first = row_of(first, slot_first)
        row_second = row_of(second, slot_second)
        index = lax.broadcasted_iota(jnp.int32, (count, count), 0)
        pick[...] = jnp.where((index == row_first) | (index == row_second), 1.0, 0.0).astype(jnp.bfloat16)
        for i in range(chunks):
            load(i).wait()

    block = out_ref.shape[0]
    value = jnp.dot(pick[pl.ds(step * block, block), :], raw[...], preferred_element_type=jnp.float32)
    mean = jnp.mean(value * value, axis=1, keepdims=True)
    out_ref[...] = (value * lax.rsqrt(mean + epsilon) * gain_ref[...]).astype(jnp.bfloat16)


def dispatch_buffer(ids_rows, gain, tokens, rows):
    count, width = tokens.shape
    steps, chunks = 2, 2
    return pl.pallas_call(
        functools.partial(dispatch_kernel, rows=rows, chunks=chunks),
        grid=(steps,),
        in_specs=[
            pl.BlockSpec((2, count), lambda i: (0, 0)),
            pl.BlockSpec((1, width), lambda i: (0, 0)),
            pl.BlockSpec(memory_space=pltpu.HBM),
        ],
        out_specs=pl.BlockSpec((count // steps, width), lambda i: (i, 0)),
        scratch_shapes=[
            pltpu.VMEM((count, width), jnp.bfloat16),
            pltpu.VMEM((count, count), jnp.bfloat16),
            pltpu.SemaphoreType.DMA((chunks,)),
        ],
        out_shape=pltpu.HBM((count, width), jnp.bfloat16),
        compiler_params=pltpu.CompilerParams(dimension_semantics=("arbitrary",), vmem_limit_bytes=58 * MIB),
        name="dispatch_buffer",
    )(ids_rows, gain, tokens)


def start_one(flag, a, b, dst, sem):
    @pl.when(flag == 1)
    def _():
        pltpu.make_async_copy(a, dst, sem).start()

    @pl.when(flag != 1)
    def _():
        pltpu.make_async_copy(b, dst, sem).start()


def activation(acts, part):
    gate_acts = acts[:, :part]
    return (gate_acts / (1.0 + jnp.exp(-gate_acts)) * acts[:, part:]).astype(jnp.bfloat16)


def halves_of(width):
    return ((0, width // 2), (width // 2, width // 2))


def split_block(rows_ref, weights, waits):
    acts = None
    for (lo, size), wait in zip(halves_of(rows_ref.shape[1]), waits):
        wait()
        term = jnp.dot(
            rows_ref[:, lo : lo + size], weights[lo : lo + size, :], preferred_element_type=jnp.float32
        )
        acts = term if acts is None else acts + term
    return acts


def early_kernel(place_ref, rows_ref, ga, gb, g1, g2, ua, ub, u1, u2, out_ref, own_ref, weights, sems):
    flag = place_ref[1]
    width, part = g1.shape

    def plain(at, lo, size, gate, up):
        for n, source in enumerate((gate, up)):
            yield (
                source.at[pl.ds(lo, size)],
                weights.at[at, pl.ds(lo, size), pl.ds(n * part, part)],
            )

    def wait_for(at, lo, size, sem):
        for n, (source, target) in enumerate(plain(at, lo, size, g1, u1)):
            pltpu.make_async_copy(source, target, sems.at[sem + n]).wait()

    for half, (lo, size) in enumerate(halves_of(width)):
        for n, (source, target) in enumerate(plain(0, lo, size, g1, u1)):
            pltpu.make_async_copy(source, target, sems.at[2 * half + n]).start()
    for n, (source, target) in enumerate(plain(1, 0, width, g2, u2)):
        pltpu.make_async_copy(source, target, sems.at[4 + n]).start()
    own_gate = own_ref.at[:, pl.ds(0, part)]
    own_up = own_ref.at[:, pl.ds(part, part)]
    start_one(flag, ga, gb, own_gate, sems.at[6])
    start_one(flag, ua, ub, own_up, sems.at[7])
    waits = [
        functools.partial(wait_for, 0, lo, size, 2 * half) for half, (lo, size) in enumerate(halves_of(width))
    ]
    out_ref[:, 0:part] = activation(split_block(rows_ref, weights.at[0], waits), part)
    wait_for(1, 0, width, 4)
    acts = jnp.dot(rows_ref[...], weights[1], preferred_element_type=jnp.float32)
    out_ref[:, part : 2 * part] = activation(acts, part)
    pltpu.make_async_copy(ga, own_gate, sems.at[6]).wait()
    pltpu.make_async_copy(ua, own_up, sems.at[7]).wait()


def own_kernel(rows_ref, weights_ref, out_ref):
    acts = jnp.dot(rows_ref[...], weights_ref[...], preferred_element_type=jnp.float32)
    out_ref[...] = activation(acts, out_ref.shape[1])


def middle_kernel(place_ref, rows_ref, ga, gb, ua, ub, out_ref, weights, sems):
    flag = place_ref[1]
    width, part = ga.shape

    def target(lo, size, n):
        return weights.at[pl.ds(lo, size), pl.ds(n * part, part)]

    def wait_for(half, lo, size):
        for n in range(2):
            pltpu.make_async_copy(ga.at[pl.ds(lo, size)], target(lo, size, n), sems.at[2 * half + n]).wait()

    waits = []
    for half, (lo, size) in enumerate(halves_of(width)):
        for n, (a, b) in enumerate(((ga, gb), (ua, ub))):
            start_one(flag, a.at[pl.ds(lo, size)], b.at[pl.ds(lo, size)], target(lo, size, n), sems.at[2 * half + n])
        waits.append(functools.partial(wait_for, half, lo, size))
    out_ref[...] = activation(split_block(rows_ref, weights, waits), part)


HBM = pl.BlockSpec(memory_space=pltpu.HBM)
ANY = pl.BlockSpec(memory_space=pl.ANY)
SMEM = pl.BlockSpec(memory_space=pltpu.SMEM)
VMEM = pl.BlockSpec(memory_space=pltpu.VMEM)


def early_hidden(place, rows, gates, ups):
    count, width = rows.shape
    part = gates[0].shape[1]
    return pl.pallas_call(
        early_kernel,
        in_specs=[SMEM, VMEM] + [ANY] * 8,
        out_specs=[VMEM, VMEM],
        scratch_shapes=[pltpu.VMEM((2, width, 2 * part), jnp.bfloat16), pltpu.SemaphoreType.DMA((8,))],
        out_shape=[pltpu.VMEM((count, 2 * part), jnp.bfloat16), pltpu.VMEM((width, 2 * part), jnp.bfloat16)],
        compiler_params=pltpu.CompilerParams(vmem_limit_bytes=32 * MIB),
        name="early_hidden",
    )(place, rows, *gates, *ups)


def own_hidden(rows, weights):
    return pl.pallas_call(
        own_kernel,
        in_specs=[VMEM, VMEM],
        out_specs=VMEM,
        out_shape=pltpu.VMEM((rows.shape[0], weights.shape[1] // 2), jnp.bfloat16),
        compiler_params=pltpu.CompilerParams(vmem_limit_bytes=32 * MIB),
        name="own_hidden",
    )(rows, weights)


def middle_hidden(place, rows, gates, ups):
    count, width = rows.shape
    part = gates[0].shape[1]
    return pl.pallas_call(
        middle_kernel,
        in_specs=[SMEM, VMEM] + [ANY] * 4,
        out_specs=VMEM,
        scratch_shapes=[pltpu.VMEM((width, 2 * part), jnp.bfloat16), pltpu.SemaphoreType.DMA((4,))],
        out_shape=pltpu.VMEM((count, part), jnp.bfloat16),
        compiler_params=pltpu.CompilerParams(vmem_limit_bytes=32 * MIB),
        name="middle_hidden",
    )(place, rows, *gates, *ups)


def late_kernel(place_ref, early_ref, middle_ref, own_ref, d0a, d0b, d1, d2, d3a, d3b, out_ref, down, hidden, out, sems, out_sems, *, cuts):
    flag = place_ref[1]
    senders, pieces, slots, piece = out_ref.shape
    part = d1.shape[0]
    size = piece // cuts
    steps = pieces * cuts

    def target(i, f):
        return down.at[pl.ds(i * part, part), pl.ds(f * size, size)]

    def source(ref, f):
        return ref.at[:, pl.ds(f * size, size)]

    for f in range(steps):
        pltpu.make_async_copy(source(d1, f), target(1, f), sems.at[4 * f + 1]).start()
        pltpu.make_async_copy(source(d2, f), target(2, f), sems.at[4 * f + 2]).start()
        start_one(flag, source(d0a, f), source(d0b, f), target(0, f), sems.at[4 * f])
        start_one(flag, source(d3a, f), source(d3b, f), target(3, f), sems.at[4 * f + 3])
    hidden[:, 0:part] = own_ref[...]
    hidden[:, part : 3 * part] = early_ref[...]
    hidden[:, 3 * part : 4 * part] = middle_ref[...]

    def store(f):
        return pltpu.make_async_copy(
            out.at[f], out_ref.at[:, f // cuts, :, pl.ds(f % cuts * size, size)], out_sems.at[f]
        )

    for f in range(steps):
        for i in range(4):
            pltpu.make_async_copy(source(d1, f), target(i, f), sems.at[4 * f + i]).wait()
        value = jnp.dot(
            hidden[...], down[:, f * size : (f + 1) * size], preferred_element_type=jnp.float32
        )
        out[f] = value.reshape(senders, slots, size).astype(jnp.bfloat16)
        store(f).start()
    for f in range(steps):
        store(f).wait()


def late_outputs(place, early, middle, own, downs, senders, pieces):
    count = early.shape[0]
    part, width = downs[0].shape
    slots = count // senders
    piece = width // pieces
    shape = (senders, pieces, slots, piece)
    cuts = 1
    return pl.pallas_call(
        functools.partial(late_kernel, cuts=cuts),
        in_specs=[SMEM, VMEM, VMEM, VMEM] + [ANY] * 6,
        out_specs=HBM,
        scratch_shapes=[
            pltpu.VMEM((4 * part, width), jnp.bfloat16),
            pltpu.VMEM((count, 4 * part), jnp.bfloat16),
            pltpu.VMEM((pieces * cuts, senders, slots, piece // cuts), jnp.bfloat16),
            pltpu.SemaphoreType.DMA((4 * pieces * cuts,)),
            pltpu.SemaphoreType.DMA((pieces * cuts,)),
        ],
        out_shape=pltpu.HBM(shape, jnp.bfloat16),
        compiler_params=pltpu.CompilerParams(vmem_limit_bytes=50 * MIB),
        name="late_outputs",
    )(place, early, middle, own, *downs)


def table_kernel(ids_ref, scores_ref, out_ref, *, rows, count_tp):
    count = ids_ref.shape[0]
    experts = 32
    first = ids_ref[:, 0:1]
    second = ids_ref[:, 1:2]
    number = lax.broadcasted_iota(jnp.int32, (count, experts), 1)
    named_first = number == first
    named_second = number == second
    named = jnp.where(named_first | named_second, 1.0, 0.0).astype(jnp.bfloat16)
    before = lax.broadcasted_iota(jnp.int32, (count, count), 1) < lax.broadcasted_iota(
        jnp.int32, (count, count), 0
    )
    ranks = jnp.dot(
        jnp.where(before, 1.0, 0.0).astype(jnp.bfloat16), named, preferred_element_type=jnp.float32
    )
    scores = scores_ref[...]
    out_ref[:, 2:4] = scores / jnp.sum(scores, axis=1, keepdims=True)
    for choice, (ids, chosen) in enumerate(((first, named_first), (second, named_second))):
        slot = jnp.sum(jnp.where(chosen, ranks, 0.0), axis=1, keepdims=True).astype(jnp.int32)
        ep, tp, row = place_of(ids, slot)
        out_ref[:, choice : choice + 1] = ((ep * count_tp + tp) * rows + row).astype(jnp.float32)


def routing_table(ids, scores, rows, count_tp):
    return pl.pallas_call(
        functools.partial(table_kernel, rows=rows, count_tp=count_tp),
        out_shape=jax.ShapeDtypeStruct((ids.shape[0], 4), jnp.float32),
        compiler_params=pltpu.CompilerParams(vmem_limit_bytes=16 * MIB),
        name="columns",
    )(ids, scores)


def combine_kernel(table_ref, returned_ref, out_ref, squares_ref):
    total = returned_ref.shape[0]
    count = table_ref.shape[0]
    index = lax.broadcasted_iota(jnp.int32, (count, total), 1)
    row = table_ref[:, 0:2].astype(jnp.int32)
    mix = table_ref[:, 2:4]
    hot = jnp.where(index == row[:, 0:1], mix[:, 0:1], jnp.where(index == row[:, 1:2], mix[:, 1:2], 0.0))
    value = jnp.dot(hot.astype(jnp.bfloat16), returned_ref[...], preferred_element_type=jnp.float32)
    out_ref[...] = value
    square = value * value
    lanes = 128
    folded = square[:, 0:lanes]
    for i in range(1, square.shape[1] // lanes):
        folded = folded + square[:, i * lanes : (i + 1) * lanes]
    squares_ref[...] = jnp.sum(folded.T, axis=0, keepdims=True)


def combine(table, returned):
    count = table.shape[0]
    piece = returned.shape[1]
    return pl.pallas_call(
        combine_kernel,
        in_specs=[VMEM, VMEM],
        out_specs=[VMEM, VMEM],
        out_shape=[
            pltpu.VMEM((count, piece), jnp.float32),
            jax.ShapeDtypeStruct((1, count), jnp.float32),
        ],
        compiler_params=pltpu.CompilerParams(vmem_limit_bytes=32 * MIB),
        name="combine",
    )(table, returned)


def scale_kernel(combined_ref, own_ref, a_ref, b_ref, c_ref, gain_ref, out_ref, *, width):
    total = own_ref[...] + a_ref[...] + b_ref[...] + c_ref[...]
    factor = lax.rsqrt(total / width + epsilon)
    count, piece = combined_ref.shape
    lanes = 128
    column = jnp.broadcast_to(factor, (lanes, count)).T
    for i in range(piece // lanes):
        at = slice(i * lanes, (i + 1) * lanes)
        out_ref[:, at] = (combined_ref[:, at] * column * gain_ref[:, at]).astype(jnp.bfloat16)


def scale(combined, squares, gain, width):
    count, piece = combined.shape
    return pl.pallas_call(
        functools.partial(scale_kernel, width=width),
        in_specs=[VMEM] * 6,
        out_specs=VMEM,
        out_shape=jax.ShapeDtypeStruct((count, piece), jnp.bfloat16),
        compiler_params=pltpu.CompilerParams(vmem_limit_bytes=16 * MIB),
        name="scale",
    )(combined, *squares, gain)


def per_device(
    tokens, in_gain, route_ids, route_scores, gate_weight, up_weight, down_weight, out_gain
):
    count_ep = lax.axis_size("ep")
    count_tp = lax.axis_size("tp")
    tok_count, full_width = tokens.shape
    part_width = full_width // count_tp
    capacity = 2 * tok_count * route_ids.shape[1] // count_ep
    rows = capacity // count_tp
    x = lax.axis_index("tp")
    core = lax.axis_index("ep") % 2
    place = jnp.stack([x, (x // 2 == core).astype(jnp.int32)]).astype(jnp.int32)

    first, second, swap = permutes(count_ep, count_tp)

    def send(weight, pairs):
        return lax.ppermute(weight, AXES, pairs)

    def spread(name, weight):
        moved = send(weight, first)
        other_own = send(weight, swap)
        other_moved = send(moved, swap)
        last = send(moved, second)
        other_last = send(last, swap)
        hold = in_vmem if name == "down" else in_hbm
        return (in_hbm(weight), in_hbm(other_own)), in_hbm(moved), in_hbm(other_moved), (hold(other_last), in_hbm(last))

    gate = spread("gate", gate_weight[0])
    up = spread("up", up_weight[0])
    down = spread("down", down_weight[0])

    buffer = dispatch_buffer(route_ids.T, in_gain[None, :], tokens, rows)
    received = lax.all_to_all(
        buffer.reshape(count_ep, rows, full_width), "ep", split_axis=0, concat_axis=0, tiled=True
    ).reshape(count_ep * rows, full_width)
    received = in_vmem(received)
    early, weights = early_hidden(place, received, (*gate[0], gate[1], gate[2]), (*up[0], up[1], up[2]))
    middle = middle_hidden(place, received, gate[3], up[3])
    own = own_hidden(received, weights)
    outputs = late_outputs(
        place, early, middle, own, (*down[0], down[1], down[2], *down[3]), count_ep, count_tp
    )
    returned = lax.all_to_all(
        outputs.reshape(count_ep * count_tp, rows, part_width), AXES, split_axis=0, concat_axis=0, tiled=True
    ).reshape(count_ep * count_tp * rows, part_width)
    table = routing_table(route_ids, route_scores, rows, count_tp)
    combined, squares = combine(table, in_vmem(returned))
    parts = [squares] + [
        lax.ppermute(squares, "tp", [(i, (i + shift) % count_tp) for i in range(count_tp)])
        for shift in range(1, count_tp)
    ]
    return scale(combined, parts, out_gain[None, :], full_width)


def solution(mesh):
    in_specs = (
        P("ep", None),
        P(),
        P("ep", None),
        P("ep", None),
        P("ep", None, "tp"),
        P("ep", None, "tp"),
        P("ep", "tp", None),
        P("tp"),
    )
    out_specs = P("ep", "tp")
    return jax.shard_map(per_device, mesh=mesh, in_specs=in_specs, out_specs=out_specs, check_vma=False)
```

```python
import functools

import jax
import jax.numpy as jnp
from jax import lax
from jax.experimental import pallas as pl
from jax.experimental.pallas import tpu as pltpu
from jax.sharding import PartitionSpec as P


epsilon = 1e-06
AXES = ("ep", "tp")
MIB = 1024 * 1024


def place_of(ids, slot):
    ep = (ids // 2) * 2 + slot % 2
    tp = (ids % 2) * 2 + (slot % 4) // 2
    return ep, tp, slot // 4


def in_vmem(value):
    return pltpu.with_memory_space_constraint(value, pltpu.VMEM)


def in_hbm(value):
    return pltpu.with_memory_space_constraint(value, pltpu.HBM)


def permutes(count_ep, count_tp):
    def dev(ep, x):
        return ep * count_tp + x

    first, second, swap = [], [], []
    for ep in range(count_ep):
        core = ep % 2
        for x in range(count_tp):
            own = x // 2 == core
            swap.append((dev(ep, x), dev(ep ^ 1, x)))
            if own:
                first.append((dev(ep, x), dev(ep, x ^ 1)))
            else:
                first.append((dev(ep, x), dev(ep ^ 1, count_tp - 1 - x)))
                second.append((dev(ep, x), dev(ep, x ^ 1)))
    return first, second, swap


def dispatch_kernel(ids_ref, gain_ref, tokens_ref, out_ref, raw, pick, sems, *, rows, chunks):
    step = pl.program_id(0)
    count, _ = raw.shape
    part = count // chunks

    def load(i):
        return pltpu.make_async_copy(
            tokens_ref.at[pl.ds(i * part, part)], raw.at[pl.ds(i * part, part)], sems.at[i]
        )

    @pl.when(step == 0)
    def _():
        for i in range(chunks):
            load(i).start()
        experts = 32
        first = ids_ref[0:1, :]
        second = ids_ref[1:2, :]
        number = lax.broadcasted_iota(jnp.int32, (experts, count), 0)
        named_first = number == first
        named_second = number == second
        named = jnp.where(named_first | named_second, 1.0, 0.0).astype(jnp.bfloat16)
        before = lax.broadcasted_iota(jnp.int32, (count, count), 0) < lax.broadcasted_iota(
            jnp.int32, (count, count), 1
        )
        ranks = jnp.dot(
            named, jnp.where(before, 1.0, 0.0).astype(jnp.bfloat16), preferred_element_type=jnp.float32
        )
        slot_first = jnp.sum(jnp.where(named_first, ranks, 0.0), axis=0, keepdims=True).astype(jnp.int32)
        slot_second = jnp.sum(jnp.where(named_second, ranks, 0.0), axis=0, keepdims=True).astype(jnp.int32)
        mine = lax.axis_index("tp")

        def row_of(ids, slot):
            ep, tp, row = place_of(ids, slot)
            return jnp.where(tp == mine, ep * rows + row, -1)

        row_first = row_of(first, slot_first)
        row_second = row_of(second, slot_second)
        index = lax.broadcasted_iota(jnp.int32, (count, count), 0)
        pick[...] = jnp.where((index == row_first) | (index == row_second), 1.0, 0.0).astype(jnp.bfloat16)
        for i in range(chunks):
            load(i).wait()

    block = out_ref.shape[0]
    value = jnp.dot(pick[pl.ds(step * block, block), :], raw[...], preferred_element_type=jnp.float32)
    mean = jnp.mean(value * value, axis=1, keepdims=True)
    out_ref[...] = (value * lax.rsqrt(mean + epsilon) * gain_ref[...]).astype(jnp.bfloat16)


def dispatch_buffer(ids_rows, gain, tokens, rows):
    count, width = tokens.shape
    steps, chunks = 2, 2
    return pl.pallas_call(
        functools.partial(dispatch_kernel, rows=rows, chunks=chunks),
        grid=(steps,),
        in_specs=[
            pl.BlockSpec((2, count), lambda i: (0, 0)),
            pl.BlockSpec((1, width), lambda i: (0, 0)),
            pl.BlockSpec(memory_space=pltpu.HBM),
        ],
        out_specs=pl.BlockSpec((count // steps, width), lambda i: (i, 0)),
        scratch_shapes=[
            pltpu.VMEM((count, width), jnp.bfloat16),
            pltpu.VMEM((count, count), jnp.bfloat16),
            pltpu.SemaphoreType.DMA((chunks,)),
        ],
        out_shape=pltpu.HBM((count, width), jnp.bfloat16),
        compiler_params=pltpu.CompilerParams(dimension_semantics=("arbitrary",), vmem_limit_bytes=58 * MIB),
        name="dispatch_buffer",
    )(ids_rows, gain, tokens)


def start_one(flag, a, b, dst, sem):
    @pl.when(flag == 1)
    def _():
        pltpu.make_async_copy(a, dst, sem).start()

    @pl.when(flag != 1)
    def _():
        pltpu.make_async_copy(b, dst, sem).start()


def activation(acts, part):
    gate_acts = acts[:, :part]
    return (gate_acts / (1.0 + jnp.exp(-gate_acts)) * acts[:, part:]).astype(jnp.bfloat16)


def halves_of(width):
    return ((0, width // 2), (width // 2, width // 2))


def split_block(rows_ref, weights, waits):
    acts = None
    for (lo, size), wait in zip(halves_of(rows_ref.shape[1]), waits):
        wait()
        term = jnp.dot(
            rows_ref[:, lo : lo + size], weights[lo : lo + size, :], preferred_element_type=jnp.float32
        )
        acts = term if acts is None else acts + term
    return acts


def early_kernel(place_ref, rows_ref, ga, gb, g1, g2, ua, ub, u1, u2, out_ref, own_ref, weights, sems):
    flag = place_ref[1]
    width, part = g1.shape

    def plain(at, lo, size, gate, up):
        for n, source in enumerate((gate, up)):
            yield (
                source.at[pl.ds(lo, size)],
                weights.at[at, pl.ds(lo, size), pl.ds(n * part, part)],
            )

    def wait_for(at, lo, size, sem):
        for n, (source, target) in enumerate(plain(at, lo, size, g1, u1)):
            pltpu.make_async_copy(source, target, sems.at[sem + n]).wait()

    for half, (lo, size) in enumerate(halves_of(width)):
        for n, (source, target) in enumerate(plain(0, lo, size, g1, u1)):
            pltpu.make_async_copy(source, target, sems.at[2 * half + n]).start()
    for n, (source, target) in enumerate(plain(1, 0, width, g2, u2)):
        pltpu.make_async_copy(source, target, sems.at[4 + n]).start()
    own_gate = own_ref.at[:, pl.ds(0, part)]
    own_up = own_ref.at[:, pl.ds(part, part)]
    start_one(flag, ga, gb, own_gate, sems.at[6])
    start_one(flag, ua, ub, own_up, sems.at[7])
    waits = [
        functools.partial(wait_for, 0, lo, size, 2 * half) for half, (lo, size) in enumerate(halves_of(width))
    ]
    out_ref[:, 0:part] = activation(split_block(rows_ref, weights.at[0], waits), part)
    wait_for(1, 0, width, 4)
    acts = jnp.dot(rows_ref[...], weights[1], preferred_element_type=jnp.float32)
    out_ref[:, part : 2 * part] = activation(acts, part)
    pltpu.make_async_copy(ga, own_gate, sems.at[6]).wait()
    pltpu.make_async_copy(ua, own_up, sems.at[7]).wait()


def own_kernel(place_ref, rows_ref, weights_ref, d0a, d0b, d1, d2, out_ref, down_ref, sems):
    part = d1.shape[0]
    start_one(place_ref[1], d0a, d0b, down_ref.at[pl.ds(0, part)], sems.at[0])
    pltpu.make_async_copy(d1, down_ref.at[pl.ds(part, part)], sems.at[1]).start()
    pltpu.make_async_copy(d2, down_ref.at[pl.ds(2 * part, part)], sems.at[2]).start()
    acts = jnp.dot(rows_ref[...], weights_ref[...], preferred_element_type=jnp.float32)
    out_ref[...] = activation(acts, out_ref.shape[1])
    for i in range(3):
        pltpu.make_async_copy(d1, down_ref.at[pl.ds(i * part, part)], sems.at[i]).wait()


def middle_kernel(place_ref, rows_ref, ga, gb, ua, ub, out_ref, weights, sems):
    flag = place_ref[1]
    width, part = ga.shape

    def target(lo, size, n):
        return weights.at[pl.ds(lo, size), pl.ds(n * part, part)]

    def wait_for(half, lo, size):
        for n in range(2):
            pltpu.make_async_copy(ga.at[pl.ds(lo, size)], target(lo, size, n), sems.at[2 * half + n]).wait()

    waits = []
    for half, (lo, size) in enumerate(halves_of(width)):
        for n, (a, b) in enumerate(((ga, gb), (ua, ub))):
            start_one(flag, a.at[pl.ds(lo, size)], b.at[pl.ds(lo, size)], target(lo, size, n), sems.at[2 * half + n])
        waits.append(functools.partial(wait_for, half, lo, size))
    out_ref[...] = activation(split_block(rows_ref, weights, waits), part)


HBM = pl.BlockSpec(memory_space=pltpu.HBM)
ANY = pl.BlockSpec(memory_space=pl.ANY)
SMEM = pl.BlockSpec(memory_space=pltpu.SMEM)
VMEM = pl.BlockSpec(memory_space=pltpu.VMEM)


def early_hidden(place, rows, gates, ups):
    count, width = rows.shape
    part = gates[0].shape[1]
    return pl.pallas_call(
        early_kernel,
        in_specs=[SMEM, VMEM] + [ANY] * 8,
        out_specs=[VMEM, VMEM],
        scratch_shapes=[pltpu.VMEM((2, width, 2 * part), jnp.bfloat16), pltpu.SemaphoreType.DMA((8,))],
        out_shape=[pltpu.VMEM((count, 2 * part), jnp.bfloat16), pltpu.VMEM((width, 2 * part), jnp.bfloat16)],
        compiler_params=pltpu.CompilerParams(vmem_limit_bytes=32 * MIB),
        name="early_hidden",
    )(place, rows, *gates, *ups)


def own_hidden(place, rows, weights, downs):
    part, width = downs[0].shape
    return pl.pallas_call(
        own_kernel,
        in_specs=[SMEM, VMEM, VMEM] + [ANY] * 4,
        out_specs=[VMEM, VMEM],
        scratch_shapes=[pltpu.SemaphoreType.DMA((3,))],
        out_shape=[
            pltpu.VMEM((rows.shape[0], part), jnp.bfloat16),
            pltpu.VMEM((3 * part, width), jnp.bfloat16),
        ],
        compiler_params=pltpu.CompilerParams(vmem_limit_bytes=32 * MIB),
        name="own_hidden",
    )(place, rows, weights, *downs)


def middle_hidden(place, rows, gates, ups):
    count, width = rows.shape
    part = gates[0].shape[1]
    return pl.pallas_call(
        middle_kernel,
        in_specs=[SMEM, VMEM] + [ANY] * 4,
        out_specs=VMEM,
        scratch_shapes=[pltpu.VMEM((width, 2 * part), jnp.bfloat16), pltpu.SemaphoreType.DMA((4,))],
        out_shape=pltpu.VMEM((count, part), jnp.bfloat16),
        compiler_params=pltpu.CompilerParams(vmem_limit_bytes=32 * MIB),
        name="middle_hidden",
    )(place, rows, *gates, *ups)


def late_kernel(place_ref, early_ref, middle_ref, own_ref, down_ref, d3a, d3b, out_ref, last, hidden, out, sems, out_sems):
    flag = place_ref[1]
    pieces, senders, slots, piece = out.shape
    part = last.shape[0]

    def columns(ref, f):
        return ref.at[:, pl.ds(f * piece, piece)]

    def store(f):
        return pltpu.make_async_copy(out.at[f], out_ref.at[:, f], out_sems.at[f])

    for f in range(pieces):
        start_one(flag, columns(d3a, f), columns(d3b, f), columns(last, f), sems.at[f])
    hidden[:, 0:part] = own_ref[...]
    hidden[:, part : 3 * part] = early_ref[...]
    for f in range(pieces):
        at = slice(f * piece, (f + 1) * piece)
        value = jnp.dot(hidden[...], down_ref[:, at], preferred_element_type=jnp.float32)
        pltpu.make_async_copy(columns(d3a, f), columns(last, f), sems.at[f]).wait()
        value = value + jnp.dot(middle_ref[...], last[:, at], preferred_element_type=jnp.float32)
        out[f] = value.reshape(senders, slots, piece).astype(jnp.bfloat16)
        store(f).start()
    for f in range(pieces):
        store(f).wait()


def late_outputs(place, early, middle, own, down, lasts, senders, pieces):
    count = early.shape[0]
    part, width = lasts[0].shape
    slots = count // senders
    piece = width // pieces
    shape = (senders, pieces, slots, piece)
    return pl.pallas_call(
        late_kernel,
        in_specs=[SMEM, VMEM, VMEM, VMEM, VMEM, ANY, ANY],
        out_specs=HBM,
        scratch_shapes=[
            pltpu.VMEM((part, width), jnp.bfloat16),
            pltpu.VMEM((count, 3 * part), jnp.bfloat16),
            pltpu.VMEM((pieces, senders, slots, piece), jnp.bfloat16),
            pltpu.SemaphoreType.DMA((pieces,)),
            pltpu.SemaphoreType.DMA((pieces,)),
        ],
        out_shape=pltpu.HBM(shape, jnp.bfloat16),
        compiler_params=pltpu.CompilerParams(vmem_limit_bytes=32 * MIB),
        name="late_outputs",
    )(place, early, middle, own, down, *lasts)


def table_kernel(ids_ref, scores_ref, out_ref, *, rows, count_tp):
    count = ids_ref.shape[0]
    experts = 32
    first = ids_ref[:, 0:1]
    second = ids_ref[:, 1:2]
    number = lax.broadcasted_iota(jnp.int32, (count, experts), 1)
    named_first = number == first
    named_second = number == second
    named = jnp.where(named_first | named_second, 1.0, 0.0).astype(jnp.bfloat16)
    before = lax.broadcasted_iota(jnp.int32, (count, count), 1) < lax.broadcasted_iota(
        jnp.int32, (count, count), 0
    )
    ranks = jnp.dot(
        jnp.where(before, 1.0, 0.0).astype(jnp.bfloat16), named, preferred_element_type=jnp.float32
    )
    scores = scores_ref[...]
    out_ref[:, 2:4] = scores / jnp.sum(scores, axis=1, keepdims=True)
    for choice, (ids, chosen) in enumerate(((first, named_first), (second, named_second))):
        slot = jnp.sum(jnp.where(chosen, ranks, 0.0), axis=1, keepdims=True).astype(jnp.int32)
        ep, tp, row = place_of(ids, slot)
        out_ref[:, choice : choice + 1] = ((ep * count_tp + tp) * rows + row).astype(jnp.float32)


def routing_table(ids, scores, rows, count_tp):
    return pl.pallas_call(
        functools.partial(table_kernel, rows=rows, count_tp=count_tp),
        out_shape=jax.ShapeDtypeStruct((ids.shape[0], 4), jnp.float32),
        compiler_params=pltpu.CompilerParams(vmem_limit_bytes=16 * MIB),
        name="columns",
    )(ids, scores)


def combine_kernel(table_ref, returned_ref, out_ref, squares_ref):
    total = returned_ref.shape[0]
    count = table_ref.shape[0]
    index = lax.broadcasted_iota(jnp.int32, (count, total), 1)
    row = table_ref[:, 0:2].astype(jnp.int32)
    mix = table_ref[:, 2:4]
    hot = jnp.where(index == row[:, 0:1], mix[:, 0:1], jnp.where(index == row[:, 1:2], mix[:, 1:2], 0.0))
    value = jnp.dot(hot.astype(jnp.bfloat16), returned_ref[...], preferred_element_type=jnp.float32)
    out_ref[...] = value
    square = value * value
    lanes = 128
    folded = square[:, 0:lanes]
    for i in range(1, square.shape[1] // lanes):
        folded = folded + square[:, i * lanes : (i + 1) * lanes]
    squares_ref[...] = jnp.sum(folded.T, axis=0, keepdims=True)


def combine(table, returned):
    count = table.shape[0]
    piece = returned.shape[1]
    return pl.pallas_call(
        combine_kernel,
        in_specs=[VMEM, VMEM],
        out_specs=[VMEM, VMEM],
        out_shape=[
            pltpu.VMEM((count, piece), jnp.float32),
            jax.ShapeDtypeStruct((1, count), jnp.float32),
        ],
        compiler_params=pltpu.CompilerParams(vmem_limit_bytes=32 * MIB),
        name="combine",
    )(table, returned)


def scale_kernel(combined_ref, own_ref, a_ref, b_ref, c_ref, gain_ref, out_ref, *, width):
    total = own_ref[...] + a_ref[...] + b_ref[...] + c_ref[...]
    factor = lax.rsqrt(total / width + epsilon)
    count, piece = combined_ref.shape
    lanes = 128
    column = jnp.broadcast_to(factor, (lanes, count)).T
    for i in range(piece // lanes):
        at = slice(i * lanes, (i + 1) * lanes)
        out_ref[:, at] = (combined_ref[:, at] * column * gain_ref[:, at]).astype(jnp.bfloat16)


def scale(combined, squares, gain, width):
    count, piece = combined.shape
    return pl.pallas_call(
        functools.partial(scale_kernel, width=width),
        in_specs=[VMEM] * 6,
        out_specs=VMEM,
        out_shape=jax.ShapeDtypeStruct((count, piece), jnp.bfloat16),
        compiler_params=pltpu.CompilerParams(vmem_limit_bytes=16 * MIB),
        name="scale",
    )(combined, *squares, gain)


def per_device(
    tokens, in_gain, route_ids, route_scores, gate_weight, up_weight, down_weight, out_gain
):
    count_ep = lax.axis_size("ep")
    count_tp = lax.axis_size("tp")
    tok_count, full_width = tokens.shape
    part_width = full_width // count_tp
    capacity = 2 * tok_count * route_ids.shape[1] // count_ep
    rows = capacity // count_tp
    x = lax.axis_index("tp")
    core = lax.axis_index("ep") % 2
    place = jnp.stack([x, (x // 2 == core).astype(jnp.int32)]).astype(jnp.int32)

    first, second, swap = permutes(count_ep, count_tp)

    def send(weight, pairs):
        return lax.ppermute(weight, AXES, pairs)

    def spread(name, weight):
        moved = send(weight, first)
        other_own = send(weight, swap)
        other_moved = send(moved, swap)
        last = send(moved, second)
        other_last = send(last, swap)
        hold = in_vmem if name == "down" else in_hbm
        return (in_hbm(weight), in_hbm(other_own)), in_hbm(moved), in_hbm(other_moved), (hold(other_last), in_hbm(last))

    gate = spread("gate", gate_weight[0])
    up = spread("up", up_weight[0])
    down = spread("down", down_weight[0])

    buffer = dispatch_buffer(route_ids.T, in_gain[None, :], tokens, rows)
    received = lax.all_to_all(
        buffer.reshape(count_ep, rows, full_width), "ep", split_axis=0, concat_axis=0, tiled=True
    ).reshape(count_ep * rows, full_width)
    received = in_vmem(received)
    early, weights = early_hidden(place, received, (*gate[0], gate[1], gate[2]), (*up[0], up[1], up[2]))
    middle = middle_hidden(place, received, gate[3], up[3])
    own, loaded = own_hidden(place, received, weights, (*down[0], down[1], down[2]))
    outputs = late_outputs(
        place, early, middle, own, loaded, down[3], count_ep, count_tp
    )
    returned = lax.all_to_all(
        outputs.reshape(count_ep * count_tp, rows, part_width), AXES, split_axis=0, concat_axis=0, tiled=True
    ).reshape(count_ep * count_tp * rows, part_width)
    table = routing_table(route_ids, route_scores, rows, count_tp)
    combined, squares = combine(table, in_vmem(returned))
    parts = [squares] + [
        lax.ppermute(squares, "tp", [(i, (i + shift) % count_tp) for i in range(count_tp)])
        for shift in range(1, count_tp)
    ]
    return scale(combined, parts, out_gain[None, :], full_width)


def solution(mesh):
    in_specs = (
        P("ep", None),
        P(),
        P("ep", None),
        P("ep", None),
        P("ep", None, "tp"),
        P("ep", None, "tp"),
        P("ep", "tp", None),
        P("tp"),
    )
    out_specs = P("ep", "tp")
    return jax.shard_map(per_device, mesh=mesh, in_specs=in_specs, out_specs=out_specs, check_vma=False)
```
